512 devices in a mesh: dp: 4 (over x), kv: 64 (over z, y), tp: 2 (over core).
Axes of the slice: x: 4, y: 4, z: 16, core: 2. Of those that a mesh axis runs over, the one named last changes fastest.
Arguments:
- tokens: bfloat16 [16, 24, 2048], P('dp'), may hold values from -6 to 6
- norm_gain: bfloat16 [2048], replicated, may hold values from 0.099609375 to 1.8984375
- w_query: bfloat16 [2048, 1024], P('kv', 'tp'), may hold values from -0.125 to 0.125
- w_key: bfloat16 [2048, 1024], P('kv', 'tp'), may hold values from -0.03125 to 0.03125
- w_value: bfloat16 [2048, 1024], P('kv', 'tp'), may hold values from -0.03125 to 0.03125
- w_forget: bfloat16 [2048, 16], P('kv', 'tp'), may hold values from -0.125 to 0.125
- forget_bias: float32 [16], P('tp'), may hold values from 0 to 4
- head_gain: bfloat16 [1024], P('tp'), may hold values from 0.099609375 to 1.8984375
- w_out: bfloat16 [1024, 2048], P('tp', 'kv'), may hold values from -0.1875 to 0.1875
- cache_keys: bfloat16 [16, 16384, 1024], P('dp', 'kv', 'tp'), may hold values from -480 to 480
- cache_values: bfloat16 [16, 16384, 1024], P('dp', 'kv', 'tp'), may hold values from -1.5 to 1.5
- cache_gates: float32 [16, 16, 16384], P('dp', 'tp', 'kv'), may hold values from -2048 to 0, as said below
- lengths: int32 [16], P('dp'), may hold values from 8192 to 16335
- accepted: int32 [16], P('dp'), may hold values from 0 to 23
- parents: int32 [16, 24], P('dp'), may hold values from -1 to 22, as said below
Outputs:
- mixed: float32 [16, 24, 2048], P('dp', None, ('kv', 'tp'))
- keys_out: bfloat16 [16, 16384, 1024], P('dp', 'kv', 'tp')
- values_out: bfloat16 [16, 16384, 1024], P('dp', 'kv', 'tp')
- gates_out: float32 [16, 16, 16384], P('dp', 'tp', 'kv')
The draws below stay inside these ranges and needn't reach their ends.
Inputs may be any that keep to these rules, and one draw needn't show every extreme that they name: parents[b, 0] = -1 and 0 <= parents[b, j] < j for every later proposal j. `cache_gates`: nonincreasing along the positions of each sequence and head.
All inputs are finite; a program needn't handle non-finite values.
Results may differ from the reference program's by a relative error of at most 0.008.
Values may be sent and summed in bfloat16 or wider, within the bound.
No kernel may reach another device: no remote copies, remote signals or barrier semaphores. Data moves between devices by JAX's collectives and lax.ppermute only.
A program may use at most 64 MiB of HBM per device.

```python
import jax
import jax.numpy as jnp
from jax import lax

D = 2048
HEADS = 16
PROP = 24
ATT_WIDTH = 1024
SEQS = 16
LENGTH = 16384


def draw_cache_keys(key, part):
    first_key = jax.random.fold_in(jax.random.fold_in(key, 11), 0)
    array_shape = (SEQS, LENGTH, ATT_WIDTH)
    values = jnp.clip(jax.random.normal(first_key, array_shape, jnp.float32), -6.0, 6.0)
    return values.astype(jnp.bfloat16)


def draw_cache_gates(key, part):
    keys = jax.random.split(jax.random.fold_in(key, 23), 5)
    share = 0.5
    quick = jax.random.uniform(keys[0], (SEQS, HEADS, 1), jnp.float32) < share
    rate_quick = 1.0 / jax.random.uniform(keys[1], (SEQS, HEADS, 1), jnp.float32, 30.0, 100.0)
    rate_slow = jax.random.uniform(keys[2], (SEQS, HEADS, 1), jnp.float32, 0.3, 1.5) / LENGTH
    rates = jnp.where(quick, rate_quick, rate_slow)
    table = jnp.exp(jax.random.uniform(keys[3], (SEQS, HEADS, 16), jnp.float32, -0.7, 0.7))
    block_index = jnp.arange(LENGTH, dtype=jnp.int32) * 16 // LENGTH
    factor = jnp.take(table, block_index, axis=2)
    rough = jax.random.uniform(keys[4], (SEQS, HEADS, LENGTH), jnp.float32, 0.3, 1.7)
    return jnp.cumsum(-rates * factor * rough, axis=2)


def draw_parents(key, part):
    stride = jax.random.randint(jax.random.fold_in(key, 37), (SEQS, PROP), 1, 5)
    indices = jnp.arange(PROP, dtype=jnp.int32)[None, :]
    return jnp.where(indices == 0, -1, jnp.maximum(indices - stride, 0)).astype(jnp.int32)


def set_ends(array, rng, smallest, top_value):
    longest = array.shape.index(max(array.shape))
    spots = []
    for shift in (0, 1):
        where = [jax.random.randint(jax.random.fold_in(rng, axis), (), 0, length) for axis, length in enumerate(array.shape)]
        where[longest] = (where[longest] + shift) % array.shape[longest]
        spots.append(tuple(where))
    return array.at[spots[0]].set(smallest).at[spots[1]].set(top_value)


def levels(stream_key, dims, shards, smallest, largest):
    loudness, own = 1.0, jax.random.fold_in(stream_key, 6)
    for axis_at, blocks in shards:
        heights = jnp.exp(jax.random.uniform(jax.random.fold_in(own, axis_at), (blocks,), jnp.float32, smallest / len(shards), largest / len(shards)))
        loudness = loudness * jnp.repeat(heights, dims[axis_at] // blocks).reshape([-1 if axis == axis_at else 1 for axis in range(len(dims))])
    return loudness


def noise(key, shape, width, bound, cuts=(), kind=jnp.bfloat16):
    result = jax.random.normal(key, shape, jnp.float32) * width
    if len(cuts) > 0:
        result = levels(key, shape, cuts, -0.22, 0.18) * result
    return jnp.clip(result, min=-bound, max=bound).astype(kind)


def setup_inputs(seed: int = 0) -> dict:
    seeds = jax.random.split(jax.random.key(seed), 16)
    tokens = noise(seeds[0], (SEQS, PROP, D), 1.0, 6.0, ((0, 4),))
    norm_gain = jnp.clip(1.0 + 0.18 * jax.random.normal(seeds[1], (D,), jnp.float32), 0.099609375, 1.8984375).astype(jnp.bfloat16)
    w_query = noise(seeds[2], (D, ATT_WIDTH), D ** -0.5, 0.125, ((0, 64), (1, 2)))
    w_key = noise(seeds[3], (D, ATT_WIDTH), (16 * D) ** -0.5, 0.03125, ((0, 64), (1, 2)))
    w_value = noise(seeds[4], (D, ATT_WIDTH), (16 * D) ** -0.5, 0.03125, ((0, 64), (1, 2)))
    w_forget = noise(seeds[5], (D, HEADS), D ** -0.5, 0.125, ((0, 64), (1, 2)))
    forget_bias = jnp.clip(4.0 * jax.random.uniform(seeds[6], (HEADS,), jnp.float32) ** levels(seeds[6], (HEADS,), ((0, 2),), -0.2, 0.2), 0.0, 4.0)
    head_gain = jnp.clip(1.0 + 0.18 * jax.random.normal(seeds[7], (ATT_WIDTH,), jnp.float32), 0.099609375, 1.8984375).astype(jnp.bfloat16)
    w_out = noise(seeds[8], (ATT_WIDTH, D), ATT_WIDTH ** -0.5, 0.1875, ((0, 2), (1, 64)))
    cache_keys = draw_cache_keys(jax.random.fold_in(seeds[15], 71), 0)
    cache_values = noise(seeds[10], (SEQS, LENGTH, ATT_WIDTH), 0.25, 1.5, ((0, 4), (1, 64), (2, 2)))
    cache_gates = draw_cache_gates(jax.random.fold_in(seeds[15], 71), 0)
    lengths = set_ends(jax.random.randint(seeds[12], (SEQS,), LENGTH // 2, LENGTH - 2 * PROP), jax.random.fold_in(seeds[12], 1), LENGTH // 2, (LENGTH - 2 * PROP) - 1).astype(jnp.int32)
    accepted = set_ends(jax.random.randint(seeds[13], (SEQS,), 0, PROP), jax.random.fold_in(seeds[13], 1), 0, PROP - 1).astype(jnp.int32)
    parents = draw_parents(jax.random.fold_in(seeds[15], 71), 0)
    return {"tokens": tokens, "norm_gain": norm_gain, "w_query": w_query, "w_key": w_key, "w_value": w_value, "w_forget": w_forget, "forget_bias": forget_bias, "head_gain": head_gain, "w_out": w_out, "cache_keys": cache_keys, "cache_values": cache_values, "cache_gates": cache_gates, "lengths": lengths, "accepted": accepted, "parents": parents}


NEG_LARGE = -1e+30
EPSILON = 1e-06

def ancestry(parents):
    prop_count = parents.shape[1]
    indices = jnp.arange(prop_count, dtype=jnp.int32)
    linked = (parents[:, :, None] == indices[None, None, :]).astype(jnp.float32)
    linked = linked + (indices[:, None] == indices[None, :]).astype(jnp.float32)[None]
    for repeat in range(prop_count.bit_length()):
        linked = jnp.minimum(jnp.einsum('bij,bjk->bik', linked, linked, precision=lax.Precision.HIGHEST), 1.0)
    return linked

def reference(tokens, norm_gain, w_query, w_key, w_value, w_forget, forget_bias, head_gain, w_out, cache_keys, cache_values, cache_gates, lengths, accepted, parents):
    seq_count, prop_count, model_width = tokens.shape
    head_count = cache_gates.shape[1]
    full_length = cache_gates.shape[2]
    head_size = cache_keys.shape[2] // head_count
    flat_rows = tokens.reshape(seq_count * prop_count, model_width).astype(jnp.float32)
    normed = (flat_rows * lax.rsqrt(lax.optimization_barrier(jnp.mean(flat_rows * flat_rows, axis=1, keepdims=True)) + EPSILON) * norm_gain.astype(jnp.float32)).astype(jnp.bfloat16)
    query = jnp.dot(normed, w_query, preferred_element_type=jnp.float32).astype(jnp.bfloat16)
    fresh_keys = jnp.dot(normed, w_key, preferred_element_type=jnp.float32).astype(jnp.bfloat16)
    fresh_values = jnp.dot(normed, w_value, preferred_element_type=jnp.float32).astype(jnp.bfloat16)
    query = query.reshape(seq_count, prop_count, head_count, head_size)
    fresh_keys = fresh_keys.reshape(seq_count, prop_count, head_count, head_size)
    fresh_values = fresh_values.reshape(seq_count, prop_count, head_count, head_size)
    log_gate = jax.nn.log_sigmoid(jnp.dot(normed, w_forget, preferred_element_type=jnp.float32) + forget_bias.astype(jnp.float32)).reshape(seq_count, prop_count, head_count)
    valid_len = (lengths + accepted).astype(jnp.int32)
    link = ancestry(parents)
    climb = jnp.einsum('bia,bah->bih', link, log_gate, precision=lax.Precision.HIGHEST)
    positions = jnp.arange(full_length, dtype=jnp.int32)
    scale = head_size ** (-0.5)
    gain_rows = head_gain.astype(jnp.float32).reshape(head_count, head_size)
    zero_index = jnp.zeros((), jnp.int32)

    def one_sequence(entry):
        q_rows, new_keys, new_values, climb_row, link_row, stored_keys, stored_values, stored_gates, valid_row = entry
        last_gate = lax.dynamic_slice_in_dim(stored_gates, valid_row - 1, 1, 1)[:, 0]
        key_rows = stored_keys.reshape(full_length, head_count, head_size).astype(jnp.float32)
        value_rows = stored_values.reshape(full_length, head_count, head_size).astype(jnp.float32)
        q_float = q_rows.astype(jnp.float32)
        far_scores = jnp.einsum('phd,chd->phc', q_float, key_rows) * scale
        far_scores = far_scores + (last_gate[None, :] + climb_row)[:, :, None] - stored_gates[None]
        far_mask = (positions < valid_row)[None, None, :]
        far_scores = jnp.where(far_mask, far_scores, NEG_LARGE)
        near_scores = jnp.einsum('phd,ahd->pha', q_float, new_keys.astype(jnp.float32)) * scale
        near_scores = near_scores + climb_row[:, :, None] - jnp.transpose(climb_row)[None]
        near_mask = (link_row > 0.5)[:, None, :]
        near_scores = jnp.where(near_mask, near_scores, NEG_LARGE)
        highest = jnp.maximum(lax.optimization_barrier(jnp.max(far_scores, axis=2)), lax.optimization_barrier(jnp.max(near_scores, axis=2)))
        far_weights = jnp.where(far_mask, jnp.exp(far_scores - highest[:, :, None]), 0.0)
        near_weights = jnp.where(near_mask, jnp.exp(near_scores - highest[:, :, None]), 0.0)
        normalizer = lax.optimization_barrier(jnp.sum(far_weights, axis=2)) + lax.optimization_barrier(jnp.sum(near_weights, axis=2))
        far_rounded = lax.optimization_barrier(far_weights.astype(jnp.bfloat16)).astype(jnp.float32)
        near_rounded = lax.optimization_barrier(near_weights.astype(jnp.bfloat16)).astype(jnp.float32)
        attended = jnp.einsum('phc,chd->phd', far_rounded, value_rows)
        attended = attended + jnp.einsum('pha,ahd->phd', near_rounded, new_values.astype(jnp.float32))
        attended = attended / normalizer[:, :, None]
        heads_out = attended * lax.rsqrt(lax.optimization_barrier(jnp.mean(attended * attended, axis=2, keepdims=True)) + EPSILON) * gain_rows[None]
        keys_out = lax.dynamic_update_slice(stored_keys, new_keys.reshape(prop_count, head_count * head_size), (valid_row, zero_index))
        values_out = lax.dynamic_update_slice(stored_values, new_values.reshape(prop_count, head_count * head_size), (valid_row, zero_index))
        gates_out = lax.dynamic_update_slice(stored_gates, last_gate[:, None] + jnp.transpose(climb_row), (zero_index, valid_row))
        return (heads_out.astype(jnp.bfloat16).reshape(prop_count, head_count * head_size), keys_out, values_out, gates_out)
    heads_all, keys_out, values_out, gates_out = lax.map(one_sequence, (query, fresh_keys, fresh_values, climb, link, cache_keys, cache_values, cache_gates, valid_len))
    flat_heads = heads_all.reshape(seq_count * prop_count, head_count * head_size)
    mixed = jnp.dot(flat_heads, w_out, preferred_element_type=jnp.float32).reshape(seq_count, prop_count, model_width)
    return (mixed, keys_out, values_out, gates_out)
```

```python
import jax
import jax.numpy as jnp
from jax import lax
from jax.experimental import pallas as pl
from jax.experimental.pallas import tpu as pltpu
from jax.sharding import Mesh
from jax.sharding import PartitionSpec as P

KV = ("kv_0", "kv_1")
KV_TP = ("kv_0", "kv_1", "tp")

NEG_LARGE = -1e30
EPSILON = 1e-06
F32 = jnp.float32
BF16 = jnp.bfloat16

GROUP = 6
SLOTS = 8
NT = (((1,), (1,)), ((), ()))
INTERPRET = False


def iota(shape, dim):
    return lax.broadcasted_iota(jnp.int32, shape, dim)


def three_parts(x):
    high = x.astype(BF16).astype(F32)
    rest = x - high
    middle = rest.astype(BF16).astype(F32)
    return high, middle, rest - middle


def pack_kernel(wq_ref, wk_ref, wv_ref, wf_ref, out_ref):
    rows = wq_ref.shape[0]
    stacked = jnp.concatenate(
        [wq_ref[...].astype(F32), wk_ref[...].astype(F32), wv_ref[...].astype(F32), jnp.zeros((rows, wq_ref.shape[1]), F32)],
        axis=0,
    )
    turned = stacked.T.reshape(out_ref.shape)
    forget = jnp.concatenate([jnp.zeros((8, 3 * rows), F32), wf_ref[...].astype(F32)], axis=1)
    lane = iota((1, 8, 128), 2)
    out_ref[...] = jnp.where(lane >= 3 * rows, forget[None], turned).astype(BF16)


def project_kernel(x_ref, tok_ref, gain_ref, bias_ref, par_ref, piece_ref, climb_ref, link_ref, wt_ref, nrm_ref):
    x = x_ref[...].astype(F32).reshape(16, 4, 8, 128)
    block = iota((128, 128), 1) // 32
    for t in range(4):
        row = None
        for n in range(4):
            moved = x[:, n].reshape(128, 128)
            if n != t:
                moved = pltpu.roll(moved, ((n - t) * 32) % 128, 1)
            row = moved if row is None else jnp.where(block == n, moved, row)
        row = row.reshape(16, 8, 128)
        for m in range(16):
            wt_ref[t * 8 : (t + 1) * 8, m * 128 : (m + 1) * 128] = row[m]
    nrm_ref[...] = jnp.zeros(nrm_ref.shape, F32)
    gain = gain_ref[...].astype(F32)
    for b in range(4):
        tok = tok_ref[b].astype(F32)
        normed = tok * lax.rsqrt(jnp.mean(tok * tok, axis=1, keepdims=True) + EPSILON) * gain
        for g in range(4):
            at = b * 32 + g * SLOTS
            nrm_ref[at : at + GROUP, :] = normed[g * GROUP : (g + 1) * GROUP]
    out = lax.dot_general(
        wt_ref[...].astype(BF16), nrm_ref[...].astype(BF16), NT, preferred_element_type=F32
    )
    piece = out[:24].reshape(3, 8, 128).astype(BF16)
    piece_ref[...] = jnp.broadcast_to(piece[None], piece_ref.shape)
    pre = out[24:] + bias_ref[...]
    log_gate = jnp.minimum(pre, 0.0) - jnp.log1p(jnp.exp(-jnp.abs(pre)))
    child = iota((128, 128), 0)
    linked = ((par_ref[...] == child) | (child == iota((128, 128), 1))).astype(F32)
    for repeat in range(5):
        low = linked.astype(BF16)
        linked = jnp.minimum(jnp.dot(low, low, preferred_element_type=F32), 1.0)
    parts = jnp.concatenate(three_parts(log_gate), axis=0).astype(BF16)
    summed = jnp.dot(parts, linked.astype(BF16), preferred_element_type=F32)
    climb_ref[...] = summed[:8] + summed[8:16] + summed[16:]
    link_ref[...] = linked.T


def slot_token(lane):
    return jnp.where(lane % SLOTS < GROUP, (lane % 32) // SLOTS * GROUP + lane % SLOTS, -100000)


def placement(b, off, rows):
    lane = iota((rows, 128), 1)
    return (iota((rows, 128), 0) - off == slot_token(lane)) & (lane // 32 == b)


def attend_kernel(len_ref, acc_ref, g_ref, k_ref, v_ref, gate_ref, kout_ref, vout_ref, out_ref, q_ref, kt_ref, vt_ref, last_ref):
    b = pl.program_id(0)
    rows = k_ref.shape[1]
    start = lax.axis_index(KV) * rows

    @pl.when(b == 0)
    def _():
        q_ref[...] = g_ref[:, 0].astype(F32).reshape(512, 128).T
        kt_ref[...] = g_ref[:, 1].astype(F32).reshape(512, 128).astype(BF16)
        vt_ref[...] = g_ref[:, 2].astype(F32).reshape(512, 128).astype(BF16)
        lane = iota((8, 128), 1)
        total = jnp.zeros((8, 128), F32)
        for s in range(4):
            at = len_ref[s] + acc_ref[s] - 1 - start
            found = jnp.sum(jnp.where(iota((8, rows), 1) == at, gate_ref[s], 0.0), axis=1, keepdims=True)
            high, middle, low = three_parts(jnp.broadcast_to(found, (8, 128)))
            value = jnp.where(lane < 32, high, jnp.where(lane < 64, middle, low))
            here = (lane % 32 == s * 8 + iota((8, 128), 0)) & (lane < 96)
            total = total + jnp.where(here, value, 0.0)
        last_ref[...] = jnp.broadcast_to(jnp.sum(total, axis=0, keepdims=True), (8, 128))

    off = len_ref[b] + acc_ref[b] - start
    gates = gate_ref[b]
    seen = iota((64, rows), 1) < off
    lane = iota((64, 128), 1)
    half = lane < 64
    part = (lane % 64) // 8
    row = iota((64, 128), 0)
    mine = (lane % 8 == row % 8) & ((lane // 64) == (row // 32))
    slot = iota((4, 8, 128), 1)
    last = last_ref[...][None]
    for p in range(4):
        q = q_ref[pl.ds(b * 32, 32), p * 128 : (p + 1) * 128]
        both = jnp.concatenate([jnp.where(half[:32], q, 0.0), jnp.where(half[:32], 0.0, q)], axis=0).astype(BF16)
        scores = lax.dot_general(
            both, k_ref[0, :, p * 128 : (p + 1) * 128], NT, preferred_element_type=F32
        ) * 0.125
        shift = jnp.concatenate(
            [jnp.broadcast_to(gates[2 * p : 2 * p + 1], (32, rows)), jnp.broadcast_to(gates[2 * p + 1 : 2 * p + 2], (32, rows))],
            axis=0,
        )
        scores = jnp.where(seen, scores - shift, NEG_LARGE)
        highest = jnp.max(scores, axis=1, keepdims=True)
        weights = jnp.where(seen, jnp.exp(scores - highest), 0.0)
        total = jnp.sum(weights, axis=1, keepdims=True)
        weighted = jnp.dot(weights.astype(BF16), v_ref[0, :, p * 128 : (p + 1) * 128], preferred_element_type=F32)
        some = total > 0.0
        weighted = weighted * jnp.where(some, 1.0 / jnp.where(some, total, 1.0), 0.0)
        level = jnp.where(some, highest + jnp.log(jnp.where(some, total, 1.0)), NEG_LARGE)
        high, middle, low = three_parts(jnp.broadcast_to(level, (64, 128)))
        value = jnp.where(part == 0, high, jnp.where(part == 1, middle, low))
        value = jnp.where(mine & (part < 3), value, 0.0)
        levels = jnp.sum((value[:32] + value[32:]).reshape(4, 8, 128), axis=1, keepdims=True)
        pair = jnp.where(half[:32], weighted[:32], weighted[32:]).reshape(4, 8, 128)
        pair = jnp.where(slot == 6, levels, jnp.where(slot == 7, last, pair))
        out_ref[p * 4 : (p + 1) * 4, 0] = pair.astype(BF16)
    landing = (off > -24) & (off < rows)

    @pl.when(jnp.logical_not(landing))
    def _():
        kout_ref[...] = k_ref[...]
        vout_ref[...] = v_ref[...]

    @pl.when(landing)
    def _():
        placed = placement(b, off, rows).astype(F32).astype(BF16)
        index = iota((rows, 512), 0)
        landed = (index >= off) & (index < off + 24)
        for source, fresh, target in ((k_ref, kt_ref, kout_ref), (v_ref, vt_ref, vout_ref)):
            written = lax.dot_general(placed, fresh[...], NT, preferred_element_type=F32)
            target[0] = jnp.where(landed, written, source[0].astype(F32)).astype(BF16)


def merge_kernel(len_ref, acc_ref, r_ref, g_ref, climb_ref, link_ref, gate_ref, gain_ref, out_ref, gout_ref, qn_ref):
    rows = gate_ref.shape[2]
    index = lax.axis_index(KV)
    start = index * rows
    p = index // 16
    group = (index // 4) % 4
    seq = index % 4
    got = r_ref[...].astype(F32)
    lane3 = iota((64, 8, 128), 2)
    keep = (lane3 % 8 == iota((64, 8, 128), 1)) & ((lane3 % 64) // 8 < 3)
    level = jnp.where(keep, got[:, 6:7, :], 0.0).reshape(512, 128).astype(BF16)
    halves = (iota((128, 128), 0) // 64 == iota((128, 128), 1) // 64).astype(F32).astype(BF16)
    level = jnp.dot(level, halves, preferred_element_type=F32).reshape(64, 8, 128)
    top = jnp.max(level, axis=0)
    scale = jnp.exp(level - top[None])
    far_sum = jnp.sum(scale, axis=0)
    far = jnp.sum(scale * got, axis=0)
    last = jnp.sum(got, axis=0)[7:8]

    lane = iota((8, 128), 1)
    half = lane < 64
    lane1 = iota((1, 128), 1)
    first = seq * 8 + 2 * p
    pick = [
        jnp.sum(jnp.where((lane1 % 32 == first + k) & (lane1 < 96), last, 0.0), axis=1, keepdims=True)
        for k in range(2)
    ]
    top = top + jnp.where(half, pick[0], pick[1])

    at = pl.multiple_of(seq * 32 + group * 8, 8)
    qn_ref[...] = g_ref[pl.ds(p * 16, 16), 0].astype(F32).reshape(128, 128).T
    keys = g_ref[pl.ds(p * 16, 16), 1].astype(F32).reshape(128, 128).astype(BF16)
    values = g_ref[pl.ds(p * 16, 16), 2].astype(F32).reshape(128, 128).astype(BF16)
    q = qn_ref[pl.ds(at, 8), :]
    both = jnp.concatenate([jnp.where(half, q, 0.0), jnp.where(half, 0.0, q)], axis=0).astype(BF16)
    near = jnp.dot(both, keys, preferred_element_type=F32) * 0.125
    climb = climb_ref[...]
    head = iota((8, 128), 0)
    climbs = [jnp.sum(jnp.where(head == 2 * p + k, climb, 0.0), axis=0, keepdims=True) for k in range(2)]
    near = near - jnp.concatenate([jnp.broadcast_to(c, (8, 128)) for c in climbs], axis=0)
    linked = link_ref[pl.ds(at, 8), :]
    linked = jnp.concatenate([linked, linked], axis=0) > 0.5
    near = jnp.where(linked, near, NEG_LARGE)
    near_top = jnp.max(near, axis=1, keepdims=True)
    near = jnp.where(linked, jnp.exp(near - near_top), 0.0)
    near_sum = jnp.sum(near, axis=1, keepdims=True)
    near = lax.dot_general(near.astype(BF16), values, NT, preferred_element_type=F32)
    near = jnp.where(half, near[:8], near[8:])
    near_top = jnp.where(half, near_top[:8], near_top[8:])
    near_sum = jnp.where(half, near_sum[:8], near_sum[8:])
    overall = jnp.maximum(top, near_top)
    far_scale = jnp.exp(top - overall)
    near_scale = jnp.exp(near_top - overall)
    attended = (far * far_scale + near * near_scale) / (far_sum * far_scale + near_sum * near_scale)
    square = attended * attended
    low = jnp.sum(jnp.where(half, square, 0.0), axis=1, keepdims=True)
    high = jnp.sum(jnp.where(half, 0.0, square), axis=1, keepdims=True)
    mean = jnp.where(half, low, high) * (1.0 / 64.0)
    gain = jnp.sum(jnp.where(iota((4, 128), 0) == p, gain_ref[...].astype(F32), 0.0), axis=0, keepdims=True)
    heads = (attended * lax.rsqrt(mean + EPSILON) * gain).astype(BF16)
    out_ref[...] = jnp.broadcast_to(heads[None], out_ref.shape)

    lane32 = iota((32, 128), 1)
    column = jnp.sum(
        jnp.where((lane32 % 32 == iota((32, 128), 0)) & (lane32 < 96), last, 0.0), axis=1, keepdims=True
    )
    parts = jnp.concatenate(three_parts(climb), axis=0).astype(BF16)
    for b in range(4):
        off = len_ref[b] + acc_ref[b] - start
        placed = placement(b, off, rows).astype(F32).astype(BF16)
        written = lax.dot_general(parts, placed, NT, preferred_element_type=F32)
        written = written[:8] + written[8:16] + written[16:] + column[b * 8 : (b + 1) * 8]
        spot = iota((8, rows), 1)
        gout_ref[b] = jnp.where((spot >= off) & (spot < off + 24), written, gate_ref[b])


def mix_kernel(g_ref, w_ref, out_ref):
    total = jnp.zeros((32, 128), F32)
    for p in range(4):
        heads = g_ref[p * 16 : (p + 1) * 16].astype(F32).reshape(128, 128).astype(BF16)
        total = total + lax.dot_general(w_ref[:, p * 128 : (p + 1) * 128], heads, NT, preferred_element_type=F32)
    out_ref[...] = total.reshape(out_ref.shape)


def finish_kernel(x_ref, out_ref):
    total = x_ref[0]
    for k in range(1, x_ref.shape[0]):
        total = total + x_ref[k]
    turned = total.T
    for g in range(4):
        for b in range(4):
            at = (g * 4 + b) * SLOTS
            out_ref[b, g * GROUP : (g + 1) * GROUP, :] = turned[at : at + GROUP]


def spread(array, axis):
    return lax.all_to_all(array, axis, split_axis=0, concat_axis=0, tiled=True)


def local(
    tokens,
    norm_gain,
    w_query,
    w_key,
    w_value,
    w_forget,
    forget_bias,
    head_gain,
    w_out,
    cache_keys,
    cache_values,
    cache_gates,
    lengths,
    accepted,
    parents,
):
    rows = cache_keys.shape[1]
    pair_count = lax.axis_size("tp")
    smem = pl.BlockSpec(memory_space=pltpu.SMEM)
    vmem = pl.BlockSpec(memory_space=pltpu.VMEM)
    kernel = lambda body, **kw: pl.pallas_call(body, interpret=INTERPRET, **kw)

    packed = kernel(pack_kernel, out_shape=jax.ShapeDtypeStruct((64, 8, 128), BF16))(
        w_query, w_key, w_value, w_forget.T
    )
    columns = spread(packed, KV)

    groups = parents.reshape(4, 4, GROUP)
    groups = jnp.where(
        groups < 0, -1, groups // GROUP * SLOTS + groups % GROUP + 32 * jnp.arange(4, dtype=jnp.int32)[:, None, None]
    )
    slots = jnp.pad(groups, ((0, 0), (0, 0), (0, SLOTS - GROUP)), constant_values=-1).reshape(1, 128)
    pieces, climb, link = kernel(
        project_kernel,
        out_shape=(
            jax.ShapeDtypeStruct((64, 3, 8, 128), BF16),
            jax.ShapeDtypeStruct((8, 128), F32),
            jax.ShapeDtypeStruct((128, 128), F32),
        ),
        scratch_shapes=[pltpu.VMEM((32, 2048), F32), pltpu.VMEM((128, 2048), F32)],
    )(columns, tokens, norm_gain.reshape(1, -1), forget_bias.reshape(8, 1), slots)
    gathered = spread(pieces, KV)

    cache_spec = pl.BlockSpec((1, rows, 512), lambda b: (b, 0, 0))
    keys_out, values_out, partial = kernel(
        attend_kernel,
        grid=(4,),
        in_specs=[smem, smem, vmem, cache_spec, cache_spec, vmem],
        out_specs=(cache_spec, cache_spec, pl.BlockSpec((16, 1, 8, 128), lambda b: (0, b, 0, 0))),
        out_shape=(
            jax.ShapeDtypeStruct(cache_keys.shape, BF16),
            jax.ShapeDtypeStruct(cache_values.shape, BF16),
            jax.ShapeDtypeStruct((16, 4, 8, 128), BF16),
        ),
        scratch_shapes=[
            pltpu.VMEM((128, 512), F32),
            pltpu.VMEM((512, 128), BF16),
            pltpu.VMEM((512, 128), BF16),
            pltpu.VMEM((8, 128), F32),
        ],
    )(lengths, accepted, gathered, cache_keys, cache_values, cache_gates)
    received = spread(partial.reshape(64, 8, 128), KV)

    heads, gates_out = kernel(
        merge_kernel,
        in_specs=[smem, smem] + [vmem] * 6,
        out_shape=(
            jax.ShapeDtypeStruct((64, 8, 128), BF16),
            jax.ShapeDtypeStruct(cache_gates.shape, F32),
        ),
        scratch_shapes=[pltpu.VMEM((128, 128), F32)],
    )(lengths, accepted, received, gathered, climb, link, cache_gates, head_gain.reshape(4, 128))
    everyone = spread(heads, KV)

    share = kernel(mix_kernel, out_shape=jax.ShapeDtypeStruct((pair_count, 32 // pair_count, 128), F32))(
        everyone, w_out.T
    )
    summed = spread(share, "tp")
    mixed = kernel(finish_kernel, out_shape=jax.ShapeDtypeStruct((4, 24, 32 // pair_count), F32))(summed)
    return (mixed, keys_out, values_out, gates_out)


def solution(mesh):
    torus = Mesh(
        mesh.devices.reshape(mesh.shape["dp"], 16, 4, mesh.shape["tp"]),
        ("dp", "kv_0", "kv_1", "tp"),
    )
    return jax.shard_map(
        local,
        mesh=torus,
        in_specs=(
            P("dp", None, None),
            P(),
            P(KV, "tp"),
            P(KV, "tp"),
            P(KV, "tp"),
            P(KV, "tp"),
            P("tp"),
            P("tp"),
            P("tp", KV),
            P("dp", KV, "tp"),
            P("dp", KV, "tp"),
            P("dp", "tp", KV),
            P("dp"),
            P("dp"),
            P("dp", None),
        ),
        out_specs=(P("dp", None, KV_TP), P("dp", KV, "tp"), P("dp", KV, "tp"), P("dp", "tp", KV)),
        check_vma=False,
    )
```

```python
import jax
import jax.numpy as jnp
from jax import lax
from jax.experimental import pallas as pl
from jax.experimental.pallas import tpu as pltpu
from jax.sharding import Mesh
from jax.sharding import PartitionSpec as P


KV = ("kv_0", "kv_1")
KV_TP = ("kv_0", "kv_1", "tp")

NEG_LARGE = -1e30
EPSILON = 1e-06
F32 = jnp.float32
BF16 = jnp.bfloat16

GROUP = 6
SLOTS = 8
NT = (((1,), (1,)), ((), ()))
INTERPRET = False


def iota(shape, dim):
    return lax.broadcasted_iota(jnp.int32, shape, dim)


def three_parts(x):
    high = x.astype(BF16).astype(F32)
    rest = x - high
    middle = rest.astype(BF16).astype(F32)
    return high, middle, rest - middle


def pack_kernel(wq_ref, wk_ref, wv_ref, wf_ref, out_ref):
    rows = wq_ref.shape[0]
    stacked = jnp.concatenate(
        [wq_ref[...].astype(F32), wk_ref[...].astype(F32), wv_ref[...].astype(F32), jnp.zeros((rows, wq_ref.shape[1]), F32)],
        axis=0,
    )
    turned = stacked.T.reshape(out_ref.shape)
    forget = jnp.concatenate([jnp.zeros((8, 3 * rows), F32), wf_ref[...].astype(F32)], axis=1)
    lane = iota((1, 8, 128), 2)
    out_ref[...] = jnp.where(lane >= 3 * rows, forget[None], turned).astype(BF16)


def normalize_kernel(tok_ref, gain_ref, par_ref, out_ref, link_ref, nrm_ref):
    nrm_ref[...] = jnp.zeros(nrm_ref.shape, F32)
    gain = gain_ref[...].astype(F32)
    for b in range(4):
        tok = tok_ref[b].astype(F32)
        normed = tok * lax.rsqrt(jnp.mean(tok * tok, axis=1, keepdims=True) + EPSILON) * gain
        for g in range(4):
            at = b * 32 + g * SLOTS
            nrm_ref[at : at + GROUP, :] = normed[g * GROUP : (g + 1) * GROUP]
    out_ref[...] = nrm_ref[...].astype(BF16)
    child = iota((128, 128), 0)
    linked = ((par_ref[...] == child) | (child == iota((128, 128), 1))).astype(F32)
    for _ in range(5):
        low = linked.astype(BF16)
        linked = jnp.minimum(jnp.dot(low, low, preferred_element_type=F32), 1.0)
    link_ref[...] = linked


def project_kernel(x_ref, nrm_ref, bias_ref, piece_ref, gate_ref, wt_ref):
    x = x_ref[...].astype(F32).reshape(16, 4, 8, 128)
    block = iota((128, 128), 1) // 32
    for t in range(4):
        row = None
        for n in range(4):
            moved = x[:, n].reshape(128, 128)
            if n != t:
                moved = pltpu.roll(moved, ((n - t) * 32) % 128, 1)
            row = moved if row is None else jnp.where(block == n, moved, row)
        row = row.reshape(16, 8, 128)
        for m in range(16):
            wt_ref[t * 8 : (t + 1) * 8, m * 128 : (m + 1) * 128] = row[m]
    out = lax.dot_general(wt_ref[...].astype(BF16), nrm_ref[...], NT, preferred_element_type=F32)
    piece = out[:24].reshape(3, 8, 128).astype(BF16)
    piece_ref[...] = jnp.broadcast_to(piece[None], piece_ref.shape)
    pre = out[24:] + bias_ref[...]
    gate_ref[...] = jnp.minimum(pre, 0.0) - jnp.log1p(jnp.exp(-jnp.abs(pre)))


def slot_token(lane):
    return jnp.where(lane % SLOTS < GROUP, (lane % 32) // SLOTS * GROUP + lane % SLOTS, -100000)


def placement(b, off, rows):
    lane = iota((rows, 128), 1)
    return (iota((rows, 128), 0) - off == slot_token(lane)) & (lane // 32 == b)


def columns_of(g_ref, n, start, count):
    parts = [g_ref[y, pl.ds(start, count), n].astype(F32) for y in range(4)]
    return jnp.stack(parts, axis=1).reshape(count * 32, 128)


def attend_kernel(len_ref, acc_ref, g_ref, k_ref, v_ref, gate_ref, out_ref, q_ref, last_ref):
    b = pl.program_id(0)
    rows = k_ref.shape[1]
    start = lax.axis_index(KV) * rows

    @pl.when(b == 0)
    def _():
        q_ref[...] = columns_of(g_ref, 0, 0, 16).T
        lane = iota((8, 128), 1)
        total = jnp.zeros((8, 128), F32)
        for s in range(4):
            at = len_ref[s] + acc_ref[s] - 1 - start
            found = jnp.sum(jnp.where(iota((8, rows), 1) == at, gate_ref[s], 0.0), axis=1, keepdims=True)
            high, middle, low = three_parts(jnp.broadcast_to(found, (8, 128)))
            value = jnp.where(lane < 32, high, jnp.where(lane < 64, middle, low))
            here = (lane % 32 == s * 8 + iota((8, 128), 0)) & (lane < 96)
            total = total + jnp.where(here, value, 0.0)
        last_ref[...] = jnp.broadcast_to(jnp.sum(total, axis=0, keepdims=True), (8, 128))

    off = len_ref[b] + acc_ref[b] - start
    gates = gate_ref[b]
    seen = iota((64, rows), 1) < off
    lane = iota((64, 128), 1)
    half = lane < 64
    part = (lane % 64) // 8
    row = iota((64, 128), 0)
    mine = (lane % 8 == row % 8) & ((lane // 64) == (row // 32))
    slot = iota((4, 8, 128), 1)
    last = last_ref[...][None]
    for p in range(4):
        q = q_ref[pl.ds(b * 32, 32), p * 128 : (p + 1) * 128]
        both = jnp.concatenate([jnp.where(half[:32], q, 0.0), jnp.where(half[:32], 0.0, q)], axis=0).astype(BF16)
        scores = lax.dot_general(
            both, k_ref[0, :, p * 128 : (p + 1) * 128], NT, preferred_element_type=F32
        ) * 0.125
        shift = jnp.concatenate(
            [jnp.broadcast_to(gates[2 * p : 2 * p + 1], (32, rows)), jnp.broadcast_to(gates[2 * p + 1 : 2 * p + 2], (32, rows))],
            axis=0,
        )
        scores = jnp.where(seen, scores - shift, NEG_LARGE)
        highest = jnp.max(scores, axis=1, keepdims=True)
        weights = jnp.where(seen, jnp.exp(scores - highest), 0.0)
        total = jnp.sum(weights, axis=1, keepdims=True)
        weighted = jnp.dot(weights.astype(BF16), v_ref[0, :, p * 128 : (p + 1) * 128], preferred_element_type=F32)
        some = total > 0.0
        weighted = weighted * jnp.where(some, 1.0 / jnp.where(some, total, 1.0), 0.0)
        level = jnp.where(some, highest + jnp.log(jnp.where(some, total, 1.0)), NEG_LARGE)
        high, middle, low = three_parts(jnp.broadcast_to(level, (64, 128)))
        value = jnp.where(part == 0, high, jnp.where(part == 1, middle, low))
        value = jnp.where(mine & (part < 3), value, 0.0)
        levels = jnp.sum((value[:32] + value[32:]).reshape(4, 8, 128), axis=1, keepdims=True)
        pair = jnp.where(half[:32], weighted[:32], weighted[32:]).reshape(4, 8, 128)
        pair = jnp.where(slot == 6, levels, jnp.where(slot == 7, last, pair))
        out_ref[p * 4 : (p + 1) * 4, 0] = pair.astype(BF16)


def write_kernel(len_ref, acc_ref, g_ref, k_ref, v_ref, kout_ref, vout_ref):
    b = pl.program_id(0)
    rows = k_ref.shape[1]
    off = len_ref[b] + acc_ref[b] - lax.axis_index(KV) * rows
    landing = (off > -24) & (off < rows)

    @pl.when(jnp.logical_not(landing))
    def _():
        kout_ref[...] = k_ref[...]
        vout_ref[...] = v_ref[...]

    @pl.when(landing)
    def _():
        placed = placement(b, off, rows).astype(F32).astype(BF16)
        index = iota((rows, 512), 0)
        landed = (index >= off) & (index < off + 24)
        for n, source, target in ((1, k_ref, kout_ref), (2, v_ref, vout_ref)):
            fresh = columns_of(g_ref, n, 0, 16).astype(BF16)
            written = lax.dot_general(placed, fresh, NT, preferred_element_type=F32)
            target[0] = jnp.where(landed, written, source[0].astype(F32)).astype(BF16)


def merger(index):
    return index // 16, (index // 4) % 4, index % 4


def climb_kernel(gate_ref, link_ref, climb_ref, turned_ref):
    link = link_ref[...]
    parts = jnp.concatenate(three_parts(gate_ref[...]), axis=0).astype(BF16)
    summed = jnp.dot(parts, link.astype(BF16), preferred_element_type=F32)
    climb_ref[...] = summed[:8] + summed[8:16] + summed[16:]
    turned_ref[...] = link.T


def near_kernel(g_ref, climb_ref, link_ref, out_ref, qn_ref):
    p, group, seq = merger(lax.axis_index(KV))
    half = iota((8, 128), 1) < 64
    at = pl.multiple_of(seq * 32 + group * 8, 8)
    climb = climb_ref[...]
    qn_ref[...] = columns_of(g_ref, 0, p * 4, 4).T
    keys = columns_of(g_ref, 1, p * 4, 4).astype(BF16)
    values = columns_of(g_ref, 2, p * 4, 4).astype(BF16)
    q = qn_ref[pl.ds(at, 8), :]
    both = jnp.concatenate([jnp.where(half, q, 0.0), jnp.where(half, 0.0, q)], axis=0).astype(BF16)
    near = jnp.dot(both, keys, preferred_element_type=F32) * 0.125
    head = iota((8, 128), 0)
    climbs = [jnp.sum(jnp.where(head == 2 * p + k, climb, 0.0), axis=0, keepdims=True) for k in range(2)]
    near = near - jnp.concatenate([jnp.broadcast_to(c, (8, 128)) for c in climbs], axis=0)
    linked = link_ref[pl.ds(at, 8), :]
    linked = jnp.concatenate([linked, linked], axis=0) > 0.5
    near = jnp.where(linked, near, NEG_LARGE)
    near_top = jnp.max(near, axis=1, keepdims=True)
    near = jnp.where(linked, jnp.exp(near - near_top), 0.0)
    near_sum = jnp.sum(near, axis=1, keepdims=True)
    near = lax.dot_general(near.astype(BF16), values, NT, preferred_element_type=F32)
    out_ref[0] = jnp.where(half, near[:8], near[8:])
    out_ref[1] = jnp.where(half, near_top[:8], near_top[8:])
    out_ref[2] = jnp.where(half, near_sum[:8], near_sum[8:])


def merge_kernel(r_ref, near_ref, gain_ref, out_ref, last_ref):
    p, _, seq = merger(lax.axis_index(KV))
    got = r_ref[...].astype(F32)
    lane3 = iota((64, 8, 128), 2)
    keep = (lane3 % 8 == iota((64, 8, 128), 1)) & ((lane3 % 64) // 8 < 3)
    level = jnp.where(keep, got[:, 6:7, :], 0.0).reshape(512, 128).astype(BF16)
    halves = (iota((128, 128), 0) // 64 == iota((128, 128), 1) // 64).astype(F32).astype(BF16)
    level = jnp.dot(level, halves, preferred_element_type=F32).reshape(64, 8, 128)
    top = jnp.max(level, axis=0)
    scale = jnp.exp(level - top[None])
    far_sum = jnp.sum(scale, axis=0)
    far = jnp.sum(scale * got, axis=0)
    whole = jnp.sum(got, axis=0)
    last_ref[...] = whole
    last = whole[7:8]

    half = iota((8, 128), 1) < 64
    lane1 = iota((1, 128), 1)
    first = seq * 8 + 2 * p
    pick = [
        jnp.sum(jnp.where((lane1 % 32 == first + k) & (lane1 < 96), last, 0.0), axis=1, keepdims=True)
        for k in range(2)
    ]
    top = top + jnp.where(half, pick[0], pick[1])
    near, near_top, near_sum = near_ref[0], near_ref[1], near_ref[2]
    overall = jnp.maximum(top, near_top)
    far_scale = jnp.exp(top - overall)
    near_scale = jnp.exp(near_top - overall)
    attended = (far * far_scale + near * near_scale) / (far_sum * far_scale + near_sum * near_scale)
    square = attended * attended
    low = jnp.sum(jnp.where(half, square, 0.0), axis=1, keepdims=True)
    high = jnp.sum(jnp.where(half, 0.0, square), axis=1, keepdims=True)
    mean = jnp.where(half, low, high) * (1.0 / 64.0)
    gain = jnp.sum(jnp.where(iota((4, 128), 0) == p, gain_ref[...].astype(F32), 0.0), axis=0, keepdims=True)
    heads = (attended * lax.rsqrt(mean + EPSILON) * gain).astype(BF16)
    out_ref[...] = jnp.broadcast_to(heads[None], out_ref.shape)


def gates_kernel(len_ref, acc_ref, last_ref, climb_ref, gate_ref, gout_ref):
    rows = gate_ref.shape[2]
    start = lax.axis_index(KV) * rows
    last = last_ref[...][7:8]
    lane = iota((32, 128), 1)
    column = jnp.sum(jnp.where((lane % 32 == iota((32, 128), 0)) & (lane < 96), last, 0.0), axis=1, keepdims=True)
    parts = jnp.concatenate(three_parts(climb_ref[...]), axis=0).astype(BF16)
    for b in range(4):
        off = len_ref[b] + acc_ref[b] - start
        placed = placement(b, off, rows).astype(F32).astype(BF16)
        written = lax.dot_general(parts, placed, NT, preferred_element_type=F32)
        written = written[:8] + written[8:16] + written[16:] + column[b * 8 : (b + 1) * 8]
        spot = iota((8, rows), 1)
        gout_ref[b] = jnp.where((spot >= off) & (spot < off + 24), written, gate_ref[b])


def mix_kernel(g_ref, w_ref, out_ref):
    total = jnp.zeros((32, 128), F32)
    for p in range(4):
        heads = g_ref[p * 16 : (p + 1) * 16].astype(F32).reshape(128, 128).astype(BF16)
        total = total + lax.dot_general(w_ref[:, p * 128 : (p + 1) * 128], heads, NT, preferred_element_type=F32)
    out_ref[...] = total.reshape(out_ref.shape)


def finish_kernel(x_ref, out_ref):
    total = x_ref[0]
    for k in range(1, x_ref.shape[0]):
        total = total + x_ref[k]
    for g in range(4):
        for b in range(4):
            at = (g * 4 + b) * SLOTS
            out_ref[b, :, g * GROUP : (g + 1) * GROUP] = total[:, at : at + GROUP]


def spread(array, axis):
    return lax.all_to_all(array, axis, split_axis=0, concat_axis=0, tiled=True)


def near_memory(shape, dtype):
    return pltpu.VMEM(shape, dtype)


def here(array):
    return pltpu.with_memory_space_constraint(array, pltpu.VMEM)


def step(
    tokens,
    norm_gain,
    w_query,
    w_key,
    w_value,
    w_forget,
    forget_bias,
    head_gain,
    w_out,
    cache_keys,
    cache_values,
    cache_gates,
    lengths,
    accepted,
    parents,
):
    rows = cache_keys.shape[1]
    pair_count = lax.axis_size("tp")
    smem = pl.BlockSpec(memory_space=pltpu.SMEM)
    vmem = pl.BlockSpec(memory_space=pltpu.VMEM)

    def kernel(body, out_shape, **kw):
        return pl.pallas_call(body, out_shape=out_shape, interpret=INTERPRET, **kw)

    packed = kernel(pack_kernel, near_memory((64, 8, 128), BF16))(w_query, w_key, w_value, w_forget.T)
    columns = spread(packed, KV)

    groups = parents.reshape(4, 4, GROUP)
    groups = jnp.where(
        groups < 0, -1, groups // GROUP * SLOTS + groups % GROUP + 32 * jnp.arange(4, dtype=jnp.int32)[:, None, None]
    )
    slots = jnp.pad(groups, ((0, 0), (0, 0), (0, SLOTS - GROUP)), constant_values=-1).reshape(1, 128)
    normed, link = kernel(
        normalize_kernel,
        (near_memory((128, 2048), BF16), near_memory((128, 128), F32)),
        scratch_shapes=[pltpu.VMEM((128, 2048), F32)],
    )(tokens, norm_gain.reshape(1, -1), slots)
    pieces, log_gate = kernel(
        project_kernel,
        (near_memory((16, 3, 8, 128), BF16), near_memory((8, 128), F32)),
        scratch_shapes=[pltpu.VMEM((32, 2048), F32)],
    )(here(columns), here(normed), forget_bias.reshape(8, 1))
    line = spread(pieces, KV[0])
    plane = spread(jnp.broadcast_to(line[None], (4, *line.shape)), KV[1])
    climb, turned = kernel(climb_kernel, (near_memory((8, 128), F32), near_memory((128, 128), F32)))(
        here(log_gate), here(link)
    )

    cache_spec = pl.BlockSpec((1, rows, 512), lambda b: (b, 0, 0))
    partial = kernel(
        attend_kernel,
        near_memory((16, 4, 8, 128), BF16),
        grid=(4,),
        in_specs=[smem, smem, vmem, cache_spec, cache_spec, vmem],
        out_specs=pl.BlockSpec((16, 1, 8, 128), lambda b: (0, b, 0, 0)),
        scratch_shapes=[pltpu.VMEM((128, 512), F32), pltpu.VMEM((8, 128), F32)],
    )(lengths, accepted, here(plane), cache_keys, cache_values, cache_gates)
    received = spread(partial.reshape(64, 8, 128), KV)
    keys_out, values_out = kernel(
        write_kernel,
        (
            jax.ShapeDtypeStruct(cache_keys.shape, BF16),
            jax.ShapeDtypeStruct(cache_values.shape, BF16),
        ),
        grid=(4,),
        in_specs=[smem, smem, vmem, cache_spec, cache_spec],
        out_specs=(cache_spec, cache_spec),
    )(lengths, accepted, here(plane), cache_keys, cache_values)
    near = kernel(
        near_kernel, near_memory((3, 8, 128), F32), scratch_shapes=[pltpu.VMEM((128, 128), F32)]
    )(here(plane), here(climb), here(turned))

    heads, last = kernel(
        merge_kernel,
        (near_memory((64, 8, 128), BF16), near_memory((8, 128), F32)),
    )(here(received), here(near), head_gain.reshape(4, 128))
    everyone = spread(heads, KV)
    gates_out = kernel(
        gates_kernel,
        jax.ShapeDtypeStruct(cache_gates.shape, F32),
        in_specs=[smem, smem] + [vmem] * 3,
    )(lengths, accepted, here(last), here(climb), cache_gates)

    share = kernel(mix_kernel, near_memory((pair_count, 32 // pair_count, 128), F32))(here(everyone), here(w_out.T))
    summed = spread(share, "tp")
    mixed = kernel(finish_kernel, jax.ShapeDtypeStruct((4, 32 // pair_count, 24), F32))(here(summed))
    mixed = jnp.swapaxes(mixed, 1, 2)
    return (mixed, keys_out, values_out, gates_out)


def solution(mesh):
    torus = Mesh(
        mesh.devices.reshape(mesh.shape["dp"], 16, 4, mesh.shape["tp"]),
        ("dp", "kv_0", "kv_1", "tp"),
    )
    return jax.shard_map(
        step,
        mesh=torus,
        in_specs=(
            P("dp", None, None),
            P(),
            P(KV, "tp"),
            P(KV, "tp"),
            P(KV, "tp"),
            P(KV, "tp"),
            P("tp"),
            P("tp"),
            P("tp", KV),
            P("dp", KV, "tp"),
            P("dp", KV, "tp"),
            P("dp", "tp", KV),
            P("dp"),
            P("dp"),
            P("dp", None),
        ),
        out_specs=(P("dp", None, KV_TP), P("dp", KV, "tp"), P("dp", KV, "tp"), P("dp", "tp", KV)),
        check_vma=False,
    )
```

```python
import jax
import jax.numpy as jnp
from jax import lax
from jax.experimental import pallas as pl
from jax.experimental.pallas import tpu as pltpu
from jax.sharding import Mesh
from jax.sharding import PartitionSpec as P


KV = ("kv_0", "kv_1")
KV_TP = ("kv_0", "kv_1", "tp")

NEG_LARGE = -1e30
EPSILON = 1e-06
F32 = jnp.float32
BF16 = jnp.bfloat16

GROUP = 6
SLOTS = 8
NT = (((1,), (1,)), ((), ()))
INTERPRET = False


def iota(shape, dim):
    return lax.broadcasted_iota(jnp.int32, shape, dim)


def three_parts(x):
    high = x.astype(BF16).astype(F32)
    rest = x - high
    middle = rest.astype(BF16).astype(F32)
    return high, middle, rest - middle


def merger(index):
    return index // 16, (index // 4) % 4, index % 4


def pack_kernel(wq_ref, wk_ref, wv_ref, wf_ref, out_ref):
    rows = wq_ref.shape[0]
    stacked = jnp.concatenate(
        [wq_ref[...].astype(F32), wk_ref[...].astype(F32), wv_ref[...].astype(F32), jnp.zeros((rows, wq_ref.shape[1]), F32)],
        axis=0,
    )
    turned = stacked.T.reshape(out_ref.shape)
    forget = jnp.concatenate([jnp.zeros((8, 3 * rows), F32), wf_ref[...].astype(F32)], axis=1)
    lane = iota((1, 8, 128), 2)
    out_ref[...] = jnp.where(lane >= 3 * rows, forget[None], turned).astype(BF16)


def prepare_kernel(
    len_ref, acc_ref, tok_ref, gain_ref, par_ref, bias_ref, gate_ref, head_gain_ref,
    out_ref, link_ref, turned_ref, off_ref, last_ref, bias_out_ref, own_gain_ref, nrm_ref,
):
    rows = gate_ref.shape[2]
    index = lax.axis_index(KV)
    start = index * rows
    nrm_ref[...] = jnp.zeros(nrm_ref.shape, F32)
    gain = gain_ref[...].astype(F32)
    for b in range(4):
        tok = tok_ref[b].astype(F32)
        normed = tok * lax.rsqrt(jnp.mean(tok * tok, axis=1, keepdims=True) + EPSILON) * gain
        for g in range(4):
            at = b * 32 + g * SLOTS
            nrm_ref[at : at + GROUP, :] = normed[g * GROUP : (g + 1) * GROUP]
    out_ref[...] = nrm_ref[...].astype(BF16)

    child = iota((128, 128), 0)
    linked = ((par_ref[...] == child) | (child == iota((128, 128), 1))).astype(F32)
    for _ in range(5):
        low = linked.astype(BF16)
        linked = jnp.minimum(jnp.dot(low, low, preferred_element_type=F32), 1.0)
    link_ref[...] = linked
    turned_ref[...] = linked.T

    lane = iota((8, 128), 1)
    row = iota((8, 128), 0)
    total = jnp.zeros((8, 128), F32)
    offsets = jnp.zeros((8, 128), jnp.int32)
    for s in range(4):
        off = len_ref[s] + acc_ref[s] - start
        offsets = jnp.where(row == s, off, offsets)
        found = jnp.sum(jnp.where(iota((8, rows), 1) == off - 1, gate_ref[s], 0.0), axis=1, keepdims=True)
        high, middle, low = three_parts(jnp.broadcast_to(found, (8, 128)))
        value = jnp.where(lane < 32, high, jnp.where(lane < 64, middle, low))
        total = total + jnp.where((lane % 32 == s * 8 + row) & (lane < 96), value, 0.0)
    off_ref[...] = offsets
    last_ref[...] = jnp.broadcast_to(jnp.sum(total, axis=0, keepdims=True), (8, 128))
    bias_out_ref[...] = jnp.broadcast_to(bias_ref[...], (8, 128))
    own = jnp.where(iota((4, 128), 0) == merger(index)[0], head_gain_ref[...].astype(F32), 0.0)
    own_gain_ref[...] = jnp.broadcast_to(jnp.sum(own, axis=0, keepdims=True), (8, 128))


def project_kernel(x_ref, nrm_ref, bias_ref, piece_ref, gate_ref, wt_ref):
    x = x_ref[...].astype(F32).reshape(16, 4, 8, 128)
    block = iota((128, 128), 1) // 32
    for t in range(4):
        row = None
        for n in range(4):
            moved = x[:, n].reshape(128, 128)
            if n != t:
                moved = pltpu.roll(moved, ((n - t) * 32) % 128, 1)
            row = moved if row is None else jnp.where(block == n, moved, row)
        row = row.reshape(16, 8, 128)
        for m in range(16):
            wt_ref[t * 8 : (t + 1) * 8, m * 128 : (m + 1) * 128] = row[m]
    out = lax.dot_general(wt_ref[...].astype(BF16), nrm_ref[...], NT, preferred_element_type=F32)
    piece = out[:24].reshape(3, 8, 128).astype(BF16)
    piece_ref[...] = jnp.broadcast_to(piece[None], piece_ref.shape)
    pre = out[24:] + bias_ref[...]
    gate_ref[...] = jnp.minimum(pre, 0.0) - jnp.log1p(jnp.exp(-jnp.abs(pre)))


def slot_token(lane):
    return jnp.where(lane % SLOTS < GROUP, (lane % 32) // SLOTS * GROUP + lane % SLOTS, -100000)


def placement(b, off, rows):
    lane = iota((rows, 128), 1)
    return (iota((rows, 128), 0) - off == slot_token(lane)) & (lane // 32 == b)


def columns_of(g_ref, n, start, count):
    parts = [g_ref[y, pl.ds(start, count), n].astype(F32) for y in range(4)]
    return jnp.stack(parts, axis=1).reshape(count * 32, 128)


def attend_kernel(
    off_ref, last_ref, g_ref, k_ref, v_ref, gate_ref, lg_ref, link_ref, turned_ref,
    out_ref, near_ref, climb_ref, q_ref,
):
    rows = k_ref.shape[1]
    q_ref[...] = columns_of(g_ref, 0, 0, 16).T
    lane = iota((64, 128), 1)
    half = lane < 64
    part = (lane % 64) // 8
    row = iota((64, 128), 0)
    mine = (lane % 8 == row % 8) & ((lane // 64) == (row // 32))
    slot = iota((4, 8, 128), 1)
    last = last_ref[...][None]
    for b in range(4):
        gates = gate_ref[b]
        seen = iota((64, rows), 1) < off_ref[b : b + 1, 0:1]
        for p in range(4):
            q = q_ref[b * 32 : (b + 1) * 32, p * 128 : (p + 1) * 128]
            both = jnp.concatenate([jnp.where(half[:32], q, 0.0), jnp.where(half[:32], 0.0, q)], axis=0).astype(BF16)
            scores = lax.dot_general(
                both, k_ref[b, :, p * 128 : (p + 1) * 128], NT, preferred_element_type=F32
            ) * 0.125
            shift = jnp.concatenate(
                [jnp.broadcast_to(gates[2 * p + k : 2 * p + k + 1], (32, rows)) for k in range(2)], axis=0
            )
            scores = jnp.where(seen, scores - shift, NEG_LARGE)
            highest = jnp.max(scores, axis=1, keepdims=True)
            weights = jnp.where(seen, jnp.exp(scores - highest), 0.0)
            total = jnp.sum(weights, axis=1, keepdims=True)
            weighted = jnp.dot(
                weights.astype(BF16), v_ref[b, :, p * 128 : (p + 1) * 128], preferred_element_type=F32
            )
            some = total > 0.0
            weighted = weighted * jnp.where(some, 1.0 / jnp.where(some, total, 1.0), 0.0)
            level = jnp.where(some, highest + jnp.log(jnp.where(some, total, 1.0)), NEG_LARGE)
            high, middle, low = three_parts(jnp.broadcast_to(level, (64, 128)))
            value = jnp.where(part == 0, high, jnp.where(part == 1, middle, low))
            value = jnp.where(mine & (part < 3), value, 0.0)
            levels = jnp.sum((value[:32] + value[32:]).reshape(4, 8, 128), axis=1, keepdims=True)
            pair = jnp.where(half[:32], weighted[:32], weighted[32:]).reshape(4, 8, 128)
            pair = jnp.where(slot == 6, levels, jnp.where(slot == 7, last, pair))
            out_ref[p * 4 : (p + 1) * 4, b] = pair.astype(BF16)

    parts = jnp.concatenate(three_parts(lg_ref[...]), axis=0).astype(BF16)
    summed = jnp.dot(parts, link_ref[...].astype(BF16), preferred_element_type=F32)
    climb = summed[:8] + summed[8:16] + summed[16:]
    climb_ref[...] = climb
    p, group, seq = merger(lax.axis_index(KV))
    half = iota((8, 128), 1) < 64
    at = pl.multiple_of(seq * 32 + group * 8, 8)
    keys = columns_of(g_ref, 1, p * 4, 4).astype(BF16)
    values = columns_of(g_ref, 2, p * 4, 4).astype(BF16)
    q = q_ref[pl.ds(at, 8), pl.ds(pl.multiple_of(p * 128, 128), 128)]
    both = jnp.concatenate([jnp.where(half, q, 0.0), jnp.where(half, 0.0, q)], axis=0).astype(BF16)
    near = jnp.dot(both, keys, preferred_element_type=F32) * 0.125
    head = iota((8, 128), 0)
    climbs = [jnp.sum(jnp.where(head == 2 * p + k, climb, 0.0), axis=0, keepdims=True) for k in range(2)]
    near = near - jnp.concatenate([jnp.broadcast_to(c, (8, 128)) for c in climbs], axis=0)
    linked = turned_ref[pl.ds(at, 8), :]
    linked = jnp.concatenate([linked, linked], axis=0) > 0.5
    near = jnp.where(linked, near, NEG_LARGE)
    near_top = jnp.max(near, axis=1, keepdims=True)
    near = jnp.where(linked, jnp.exp(near - near_top), 0.0)
    near_sum = jnp.sum(near, axis=1, keepdims=True)
    near = lax.dot_general(near.astype(BF16), values, NT, preferred_element_type=F32)
    near_ref[0] = jnp.where(half, near[:8], near[8:])
    near_ref[1] = jnp.where(half, near_top[:8], near_top[8:])
    near_ref[2] = jnp.where(half, near_sum[:8], near_sum[8:])


def write_kernel(len_ref, acc_ref, g_ref, k_ref, v_ref, kout_ref, vout_ref):
    b = pl.program_id(0)
    rows = k_ref.shape[1]
    off = len_ref[b] + acc_ref[b] - lax.axis_index(KV) * rows
    landing = (off > -24) & (off < rows)

    @pl.when(jnp.logical_not(landing))
    def _():
        kout_ref[...] = k_ref[...]
        vout_ref[...] = v_ref[...]

    @pl.when(landing)
    def _():
        placed = placement(b, off, rows).astype(F32).astype(BF16)
        index = iota((rows, 512), 0)
        landed = (index >= off) & (index < off + 24)
        for n, source, target in ((1, k_ref, kout_ref), (2, v_ref, vout_ref)):
            fresh = columns_of(g_ref, n, 0, 16).astype(BF16)
            written = lax.dot_general(placed, fresh, NT, preferred_element_type=F32)
            target[0] = jnp.where(landed, written, source[0].astype(F32)).astype(BF16)


def merge_kernel(r_ref, near_ref, gain_ref, out_ref, last_ref):
    p, _, seq = merger(lax.axis_index(KV))
    got = r_ref[...].astype(F32)
    lane3 = iota((64, 8, 128), 2)
    keep = (lane3 % 8 == iota((64, 8, 128), 1)) & ((lane3 % 64) // 8 < 3)
    level = jnp.where(keep, got[:, 6:7, :], 0.0).reshape(512, 128).astype(BF16)
    halves = (iota((128, 128), 0) // 64 == iota((128, 128), 1) // 64).astype(F32).astype(BF16)
    level = jnp.dot(level, halves, preferred_element_type=F32).reshape(64, 8, 128)
    top = jnp.max(level, axis=0)
    scale = jnp.exp(level - top[None])
    far_sum = jnp.sum(scale, axis=0)
    far = jnp.sum(scale * got, axis=0)
    whole = jnp.sum(got, axis=0)
    last_ref[...] = whole
    last = whole[7:8]

    half = iota((8, 128), 1) < 64
    lane1 = iota((1, 128), 1)
    first = seq * 8 + 2 * p
    pick = [
        jnp.sum(jnp.where((lane1 % 32 == first + k) & (lane1 < 96), last, 0.0), axis=1, keepdims=True)
        for k in range(2)
    ]
    top = top + jnp.where(half, pick[0], pick[1])
    near, near_top, near_sum = near_ref[0], near_ref[1], near_ref[2]
    overall = jnp.maximum(top, near_top)
    far_scale = jnp.exp(top - overall)
    near_scale = jnp.exp(near_top - overall)
    attended = (far * far_scale + near * near_scale) / (far_sum * far_scale + near_sum * near_scale)
    square = attended * attended
    low = jnp.sum(jnp.where(half, square, 0.0), axis=1, keepdims=True)
    high = jnp.sum(jnp.where(half, 0.0, square), axis=1, keepdims=True)
    mean = jnp.where(half, low, high) * (1.0 / 64.0)
    heads = (attended * lax.rsqrt(mean + EPSILON) * gain_ref[...]).astype(BF16)
    out_ref[...] = jnp.broadcast_to(heads[None], out_ref.shape)


def gates_kernel(off_ref, last_ref, climb_ref, gate_ref, gout_ref):
    rows = gate_ref.shape[2]
    last = last_ref[...][7:8]
    lane = iota((32, 128), 1)
    column = jnp.sum(jnp.where((lane % 32 == iota((32, 128), 0)) & (lane < 96), last, 0.0), axis=1, keepdims=True)
    parts = jnp.concatenate(three_parts(climb_ref[...]), axis=0).astype(BF16)
    for b in range(4):
        off = off_ref[b : b + 1, 0:1]
        placed = placement(b, off, rows).astype(F32).astype(BF16)
        written = lax.dot_general(parts, placed, NT, preferred_element_type=F32)
        written = written[:8] + written[8:16] + written[16:] + column[b * 8 : (b + 1) * 8]
        spot = iota((8, rows), 1)
        gout_ref[b] = jnp.where((spot >= off) & (spot < off + 24), written, gate_ref[b])


def mix_kernel(g_ref, w_ref, out_ref):
    total = jnp.zeros((32, 128), F32)
    for p in range(4):
        heads = g_ref[p * 16 : (p + 1) * 16].astype(F32).reshape(128, 128).astype(BF16)
        total = total + lax.dot_general(w_ref[:, p * 128 : (p + 1) * 128], heads, NT, preferred_element_type=F32)
    out_ref[...] = total.reshape(out_ref.shape)


def finish_kernel(x_ref, out_ref):
    width = out_ref.shape[1]
    own = pl.multiple_of(lax.axis_index("tp") * width, width)
    total = x_ref[0, pl.ds(own, width), :]
    for k in range(1, x_ref.shape[0]):
        total = total + x_ref[k, pl.ds(own, width), :]
    for g in range(4):
        for b in range(4):
            at = (g * 4 + b) * SLOTS
            out_ref[b, :, g * GROUP : (g + 1) * GROUP] = total[:, at : at + GROUP]


def spread(array, axis):
    return lax.all_to_all(array, axis, split_axis=0, concat_axis=0, tiled=True)


def near_memory(shape, dtype):
    return pltpu.VMEM(shape, dtype)


def here(array):
    return pltpu.with_memory_space_constraint(array, pltpu.VMEM)


def step(
    tokens,
    norm_gain,
    w_query,
    w_key,
    w_value,
    w_forget,
    forget_bias,
    head_gain,
    w_out,
    cache_keys,
    cache_values,
    cache_gates,
    lengths,
    accepted,
    parents,
):
    rows = cache_keys.shape[1]
    pair_count = lax.axis_size("tp")
    smem = pl.BlockSpec(memory_space=pltpu.SMEM)
    vmem = pl.BlockSpec(memory_space=pltpu.VMEM)

    def kernel(body, out_shape, **kw):
        return pl.pallas_call(body, out_shape=out_shape, interpret=INTERPRET, **kw)

    packed = kernel(pack_kernel, near_memory((64, 8, 128), BF16))(w_query, w_key, w_value, w_forget.T)
    columns = spread(packed, KV)

    groups = parents.reshape(4, 4, GROUP)
    groups = jnp.where(
        groups < 0, -1, groups // GROUP * SLOTS + groups % GROUP + 32 * jnp.arange(4, dtype=jnp.int32)[:, None, None]
    )
    slots = jnp.pad(groups, ((0, 0), (0, 0), (0, SLOTS - GROUP)), constant_values=-1).reshape(1, 128)
    gates = here(cache_gates)
    keys = here(cache_keys)
    values = here(cache_values)
    small = near_memory((8, 128), F32)
    normed, link, turned, offsets, last_part, bias, own_gain = kernel(
        prepare_kernel,
        (
            near_memory((128, 2048), BF16),
            near_memory((128, 128), F32),
            near_memory((128, 128), F32),
            near_memory((8, 128), jnp.int32),
            small,
            small,
            small,
        ),
        in_specs=[smem, smem] + [vmem] * 6,
        scratch_shapes=[pltpu.VMEM((128, 2048), F32)],
    )(
        lengths,
        accepted,
        tokens,
        norm_gain.reshape(1, -1),
        slots,
        forget_bias.reshape(8, 1),
        gates,
        head_gain.reshape(4, 128),
    )
    pieces, log_gate = kernel(
        project_kernel,
        (near_memory((16, 3, 8, 128), BF16), small),
        scratch_shapes=[pltpu.VMEM((32, 2048), F32)],
    )(here(columns), here(normed), here(bias))
    line = spread(pieces, KV[0])
    plane = here(spread(jnp.broadcast_to(line[None], (4, *line.shape)), KV[1]))

    partial, near, climb = kernel(
        attend_kernel,
        (near_memory((16, 4, 8, 128), BF16), near_memory((3, 8, 128), F32), small),
        scratch_shapes=[pltpu.VMEM((128, 512), F32)],
    )(
        here(offsets),
        here(last_part),
        plane,
        keys,
        values,
        gates,
        here(log_gate),
        here(link),
        here(turned),
    )
    received = spread(partial.reshape(64, 8, 128), KV)
    heads, last = kernel(merge_kernel, (near_memory((64, 8, 128), BF16), small))(
        here(received), here(near), here(own_gain)
    )
    everyone = spread(heads, KV)
    cache_spec = pl.BlockSpec((1, rows, 512), lambda b: (b, 0, 0))
    keys_out, values_out = kernel(
        write_kernel,
        (
            jax.ShapeDtypeStruct(cache_keys.shape, BF16),
            jax.ShapeDtypeStruct(cache_values.shape, BF16),
        ),
        grid=(4,),
        in_specs=[smem, smem, vmem, cache_spec, cache_spec],
        out_specs=(cache_spec, cache_spec),
    )(lengths, accepted, plane, cache_keys, cache_values)
    gates_out = kernel(gates_kernel, jax.ShapeDtypeStruct(cache_gates.shape, F32))(
        here(offsets), here(last), here(climb), gates
    )

    share = kernel(mix_kernel, near_memory((32, 128), F32))(here(everyone), here(w_out.T))
    shares = lax.all_gather(share, "tp")
    mixed = kernel(finish_kernel, jax.ShapeDtypeStruct((4, 32 // pair_count, 24), F32))(here(shares))
    mixed = jnp.swapaxes(mixed, 1, 2)
    return (mixed, keys_out, values_out, gates_out)


def solution(mesh):
    torus = Mesh(
        mesh.devices.reshape(mesh.shape["dp"], 16, 4, mesh.shape["tp"]),
        ("dp", "kv_0", "kv_1", "tp"),
    )
    return jax.shard_map(
        step,
        mesh=torus,
        in_specs=(
            P("dp", None, None),
            P(),
            P(KV, "tp"),
            P(KV, "tp"),
            P(KV, "tp"),
            P(KV, "tp"),
            P("tp"),
            P("tp"),
            P("tp", KV),
            P("dp", KV, "tp"),
            P("dp", KV, "tp"),
            P("dp", "tp", KV),
            P("dp"),
            P("dp"),
            P("dp", None),
        ),
        out_specs=(P("dp", None, KV_TP), P("dp", KV, "tp"), P("dp", KV, "tp"), P("dp", "tp", KV)),
        check_vma=False,
    )
```

```python
import jax
import jax.numpy as jnp
from jax import lax
from jax.experimental import pallas as pl
from jax.experimental.pallas import tpu as pltpu
from jax.sharding import Mesh
from jax.sharding import PartitionSpec as P


KV = ("kv_0", "kv_1")
KV_TP = ("kv_0", "kv_1", "tp")

NEG_LARGE = -1e30
EPSILON = 1e-06
F32 = jnp.float32
BF16 = jnp.bfloat16

GROUP = 6
SLOTS = 8
NT = (((1,), (1,)), ((), ()))
INTERPRET = False


def iota(shape, dim):
    return lax.broadcasted_iota(jnp.int32, shape, dim)


def three_parts(x):
    high = x.astype(BF16).astype(F32)
    rest = x - high
    middle = rest.astype(BF16).astype(F32)
    return high, middle, rest - middle


def merger(index):
    return index // 16, (index // 4) % 4, index % 4


def pack_kernel(wq_ref, wk_ref, wv_ref, wf_ref, out_ref):
    rows = wq_ref.shape[0]
    stacked = jnp.concatenate(
        [wq_ref[...].astype(F32), wk_ref[...].astype(F32), wv_ref[...].astype(F32), jnp.zeros((rows, wq_ref.shape[1]), F32)],
        axis=0,
    )
    turned = stacked.T.reshape(out_ref.shape)
    forget = jnp.concatenate([jnp.zeros((8, 3 * rows), F32), wf_ref[...].astype(F32)], axis=1)
    lane = iota((1, 8, 128), 2)
    out_ref[...] = jnp.where(lane >= 3 * rows, forget[None], turned).astype(BF16)


def prepare_kernel(
    len_ref, acc_ref, tok_ref, gain_ref, par_ref, bias_ref, gate_ref, head_gain_ref,
    out_ref, link_ref, turned_ref, off_ref, last_ref, bias_out_ref, own_gain_ref, nrm_ref,
):
    rows = gate_ref.shape[2]
    index = lax.axis_index(KV)
    start = index * rows
    nrm_ref[...] = jnp.zeros(nrm_ref.shape, F32)
    gain = gain_ref[...].astype(F32)
    for b in range(4):
        tok = tok_ref[b].astype(F32)
        normed = tok * lax.rsqrt(jnp.mean(tok * tok, axis=1, keepdims=True) + EPSILON) * gain
        for g in range(4):
            at = b * 32 + g * SLOTS
            nrm_ref[at : at + GROUP, :] = normed[g * GROUP : (g + 1) * GROUP]
    out_ref[...] = nrm_ref[...].astype(BF16)

    child = iota((128, 128), 0)
    linked = ((par_ref[...] == child) | (child == iota((128, 128), 1))).astype(F32)
    for _ in range(5):
        low = linked.astype(BF16)
        linked = jnp.minimum(jnp.dot(low, low, preferred_element_type=F32), 1.0)
    link_ref[...] = linked
    turned_ref[...] = linked.T

    lane = iota((8, 128), 1)
    row = iota((8, 128), 0)
    total = jnp.zeros((8, 128), F32)
    offsets = jnp.zeros((8, 128), jnp.int32)
    for s in range(4):
        off = len_ref[s] + acc_ref[s] - start
        offsets = jnp.where(row == s, off, offsets)
        found = jnp.sum(jnp.where(iota((8, rows), 1) == off - 1, gate_ref[s], 0.0), axis=1, keepdims=True)
        high, middle, low = three_parts(jnp.broadcast_to(found, (8, 128)))
        value = jnp.where(lane < 32, high, jnp.where(lane < 64, middle, low))
        total = total + jnp.where((lane % 32 == s * 8 + row) & (lane < 96), value, 0.0)
    off_ref[...] = offsets
    last_ref[...] = jnp.broadcast_to(jnp.sum(total, axis=0, keepdims=True), (8, 128))
    bias_out_ref[...] = jnp.broadcast_to(bias_ref[...], (8, 128))
    own = jnp.where(iota((4, 128), 0) == merger(index)[0], head_gain_ref[...].astype(F32), 0.0)
    own_gain_ref[...] = jnp.broadcast_to(jnp.sum(own, axis=0, keepdims=True), (8, 128))


def project_kernel(x_ref, nrm_ref, bias_ref, piece_ref, gate_ref, wt_ref):
    x = x_ref[...].astype(F32).reshape(16, 4, 8, 128)
    block = iota((128, 128), 1) // 32
    for t in range(4):
        row = None
        for n in range(4):
            moved = x[:, n].reshape(128, 128)
            if n != t:
                moved = pltpu.roll(moved, ((n - t) * 32) % 128, 1)
            row = moved if row is None else jnp.where(block == n, moved, row)
        row = row.reshape(16, 8, 128)
        for m in range(16):
            wt_ref[t * 8 : (t + 1) * 8, m * 128 : (m + 1) * 128] = row[m]
    out = lax.dot_general(wt_ref[...].astype(BF16), nrm_ref[...], NT, preferred_element_type=F32)
    piece = out[:24].reshape(3, 8, 128).astype(BF16)
    piece_ref[...] = jnp.broadcast_to(piece[None], piece_ref.shape)
    pre = out[24:] + bias_ref[...]
    gate_ref[...] = jnp.minimum(pre, 0.0) - jnp.log1p(jnp.exp(-jnp.abs(pre)))


def slot_token(lane):
    return jnp.where(lane % SLOTS < GROUP, (lane % 32) // SLOTS * GROUP + lane % SLOTS, -100000)


def placement(b, off, rows):
    lane = iota((rows, 128), 1)
    return (iota((rows, 128), 0) - off == slot_token(lane)) & (lane // 32 == b)


def columns_of(g_ref, n, start, count):
    parts = [g_ref[y, pl.ds(start, count), n].astype(F32) for y in range(4)]
    return jnp.stack(parts, axis=1).reshape(count * 32, 128)


def attend_kernel(
    off_ref, last_ref, g_ref, k_ref, v_ref, gate_ref, lg_ref, link_ref, turned_ref,
    out_ref, near_ref, climb_ref, q_ref,
):
    rows = k_ref.shape[1]
    q_ref[...] = columns_of(g_ref, 0, 0, 16).T * 0.125
    half = iota((32, 128), 1) < 64
    lane = iota((64, 128), 1)
    row = iota((64, 128), 0)
    mine = (lane % 8 == row % 8) & ((lane // 64) == (row // 32))
    part = (iota((4, 8, 128), 2) % 64) // 8
    slot = iota((4, 8, 128), 1)
    last = last_ref[...][None]

    def scores_of(b):
        found = []
        for p in range(4):
            q = q_ref[b * 32 : (b + 1) * 32, p * 128 : (p + 1) * 128]
            both = jnp.concatenate([jnp.where(half, q, 0.0), jnp.where(half, 0.0, q)], axis=0).astype(BF16)
            found.append(
                lax.dot_general(both, k_ref[b, :, p * 128 : (p + 1) * 128], NT, preferred_element_type=F32)
            )
        return found

    ahead = scores_of(0)
    for b in range(4):
        scores, ahead = ahead, scores_of(b + 1) if b < 3 else None
        off = off_ref[b : b + 1, 0:1]
        gates = jnp.where(iota((8, rows), 1) < off, gate_ref[b], -NEG_LARGE)
        for p in range(4):
            shifts = [jnp.broadcast_to(gates[2 * p + k : 2 * p + k + 1], (32, rows)) for k in range(2)]
            shifted = scores[p] - jnp.concatenate(shifts, axis=0)
            highest = jnp.max(shifted, axis=1, keepdims=True)
            weights = jnp.exp(shifted - highest)
            total = jnp.sum(weights, axis=1, keepdims=True)
            weighted = jnp.dot(
                weights.astype(BF16), v_ref[b, :, p * 128 : (p + 1) * 128], preferred_element_type=F32
            )
            weighted = weighted * (1.0 / total)
            level = jnp.where(mine, highest + jnp.log(total), 0.0)
            level = jnp.sum((level[:32] + level[32:]).reshape(4, 8, 128), axis=1, keepdims=True)
            level = jnp.broadcast_to(jnp.where(off > 0, level, NEG_LARGE), (4, 8, 128))
            high, middle, low = three_parts(level)
            level = jnp.where(part == 0, high, jnp.where(part == 1, middle, low))
            pair = jnp.where(half, weighted[:32], weighted[32:]).reshape(4, 8, 128)
            pair = jnp.where(slot == 6, level, jnp.where(slot == 7, last, pair))
            out_ref[p * 4 : (p + 1) * 4, b] = pair.astype(BF16)

    parts = jnp.concatenate(three_parts(lg_ref[...]), axis=0).astype(BF16)
    summed = jnp.dot(parts, link_ref[...].astype(BF16), preferred_element_type=F32)
    climb = summed[:8] + summed[8:16] + summed[16:]
    climb_ref[...] = climb
    p, group, seq = merger(lax.axis_index(KV))
    half = iota((8, 128), 1) < 64
    at = pl.multiple_of(seq * 32 + group * 8, 8)
    keys = columns_of(g_ref, 1, p * 4, 4).astype(BF16)
    values = columns_of(g_ref, 2, p * 4, 4).astype(BF16)
    q = q_ref[pl.ds(at, 8), pl.ds(pl.multiple_of(p * 128, 128), 128)]
    both = jnp.concatenate([jnp.where(half, q, 0.0), jnp.where(half, 0.0, q)], axis=0).astype(BF16)
    near = jnp.dot(both, keys, preferred_element_type=F32)
    head = iota((8, 128), 0)
    climbs = [jnp.sum(jnp.where(head == 2 * p + k, climb, 0.0), axis=0, keepdims=True) for k in range(2)]
    near = near - jnp.concatenate([jnp.broadcast_to(c, (8, 128)) for c in climbs], axis=0)
    linked = turned_ref[pl.ds(at, 8), :]
    linked = jnp.concatenate([linked, linked], axis=0) > 0.5
    near = jnp.where(linked, near, NEG_LARGE)
    near_top = jnp.max(near, axis=1, keepdims=True)
    near = jnp.where(linked, jnp.exp(near - near_top), 0.0)
    near_sum = jnp.sum(near, axis=1, keepdims=True)
    near = lax.dot_general(near.astype(BF16), values, NT, preferred_element_type=F32)
    near_ref[0] = jnp.where(half, near[:8], near[8:])
    near_ref[1] = jnp.where(half, near_top[:8], near_top[8:])
    near_ref[2] = jnp.where(half, near_sum[:8], near_sum[8:])


def write_kernel(len_ref, acc_ref, g_ref, k_ref, v_ref, kout_ref, vout_ref):
    b = pl.program_id(0)
    rows = k_ref.shape[1]
    off = len_ref[b] + acc_ref[b] - lax.axis_index(KV) * rows
    landing = (off > -24) & (off < rows)

    @pl.when(jnp.logical_not(landing))
    def _():
        kout_ref[...] = k_ref[...]
        vout_ref[...] = v_ref[...]

    @pl.when(landing)
    def _():
        placed = placement(b, off, rows).astype(F32).astype(BF16)
        index = iota((rows, 512), 0)
        landed = (index >= off) & (index < off + 24)
        for n, source, target in ((1, k_ref, kout_ref), (2, v_ref, vout_ref)):
            fresh = columns_of(g_ref, n, 0, 16).astype(BF16)
            written = lax.dot_general(placed, fresh, NT, preferred_element_type=F32)
            target[0] = jnp.where(landed, written, source[0].astype(F32)).astype(BF16)


def merge_kernel(r_ref, near_ref, gain_ref, out_ref, last_ref):
    p, _, seq = merger(lax.axis_index(KV))
    got = r_ref[...].astype(F32)
    lane3 = iota((64, 8, 128), 2)
    keep = (lane3 % 8 == iota((64, 8, 128), 1)) & ((lane3 % 64) // 8 < 3)
    level = jnp.where(keep, got[:, 6:7, :], 0.0).reshape(512, 128).astype(BF16)
    halves = (iota((128, 128), 0) // 64 == iota((128, 128), 1) // 64).astype(F32).astype(BF16)
    level = jnp.dot(level, halves, preferred_element_type=F32).reshape(64, 8, 128)
    top = jnp.max(level, axis=0)
    scale = jnp.exp(level - top[None])
    far_sum = jnp.sum(scale, axis=0)
    far = jnp.sum(scale * got, axis=0)
    whole = jnp.sum(got, axis=0)
    last_ref[...] = whole
    last = whole[7:8]

    half = iota((8, 128), 1) < 64
    lane1 = iota((1, 128), 1)
    first = seq * 8 + 2 * p
    pick = [
        jnp.sum(jnp.where((lane1 % 32 == first + k) & (lane1 < 96), last, 0.0), axis=1, keepdims=True)
        for k in range(2)
    ]
    top = top + jnp.where(half, pick[0], pick[1])
    near, near_top, near_sum = near_ref[0], near_ref[1], near_ref[2]
    overall = jnp.maximum(top, near_top)
    far_scale = jnp.exp(top - overall)
    near_scale = jnp.exp(near_top - overall)
    attended = (far * far_scale + near * near_scale) / (far_sum * far_scale + near_sum * near_scale)
    square = attended * attended
    low = jnp.sum(jnp.where(half, square, 0.0), axis=1, keepdims=True)
    high = jnp.sum(jnp.where(half, 0.0, square), axis=1, keepdims=True)
    mean = jnp.where(half, low, high) * (1.0 / 64.0)
    heads = (attended * lax.rsqrt(mean + EPSILON) * gain_ref[...]).astype(BF16)
    out_ref[...] = jnp.broadcast_to(heads[None], out_ref.shape)


def gates_kernel(off_ref, last_ref, climb_ref, gate_ref, gout_ref):
    rows = gate_ref.shape[2]
    last = last_ref[...][7:8]
    lane = iota((32, 128), 1)
    column = jnp.sum(jnp.where((lane % 32 == iota((32, 128), 0)) & (lane < 96), last, 0.0), axis=1, keepdims=True)
    parts = jnp.concatenate(three_parts(climb_ref[...]), axis=0).astype(BF16)
    for b in range(4):
        off = off_ref[b : b + 1, 0:1]
        placed = placement(b, off, rows).astype(F32).astype(BF16)
        written = lax.dot_general(parts, placed, NT, preferred_element_type=F32)
        written = written[:8] + written[8:16] + written[16:] + column[b * 8 : (b + 1) * 8]
        spot = iota((8, rows), 1)
        gout_ref[b] = jnp.where((spot >= off) & (spot < off + 24), written, gate_ref[b])


def mix_kernel(g_ref, w_ref, out_ref):
    total = jnp.zeros((32, 128), F32)
    for p in range(4):
        heads = g_ref[p * 16 : (p + 1) * 16].astype(F32).reshape(128, 128).astype(BF16)
        total = total + lax.dot_general(w_ref[:, p * 128 : (p + 1) * 128], heads, NT, preferred_element_type=F32)
    out_ref[...] = total.reshape(out_ref.shape)


def finish_kernel(x_ref, out_ref):
    width = out_ref.shape[1]
    own = pl.multiple_of(lax.axis_index("tp") * width, width)
    total = x_ref[0, pl.ds(own, width), :]
    for k in range(1, x_ref.shape[0]):
        total = total + x_ref[k, pl.ds(own, width), :]
    for g in range(4):
        for b in range(4):
            at = (g * 4 + b) * SLOTS
            out_ref[b, :, g * GROUP : (g + 1) * GROUP] = total[:, at : at + GROUP]


def spread(array, axis):
    return lax.all_to_all(array, axis, split_axis=0, concat_axis=0, tiled=True)


def near_memory(shape, dtype):
    return pltpu.VMEM(shape, dtype)


def here(array):
    return pltpu.with_memory_space_constraint(array, pltpu.VMEM)


def step(
    tokens,
    norm_gain,
    w_query,
    w_key,
    w_value,
    w_forget,
    forget_bias,
    head_gain,
    w_out,
    cache_keys,
    cache_values,
    cache_gates,
    lengths,
    accepted,
    parents,
):
    rows = cache_keys.shape[1]
    pair_count = lax.axis_size("tp")
    smem = pl.BlockSpec(memory_space=pltpu.SMEM)
    vmem = pl.BlockSpec(memory_space=pltpu.VMEM)

    def kernel(body, out_shape, **kw):
        return pl.pallas_call(body, out_shape=out_shape, interpret=INTERPRET, **kw)

    packed = kernel(pack_kernel, near_memory((64, 8, 128), BF16))(w_query, w_key, w_value, w_forget.T)
    columns = spread(packed, KV)

    groups = parents.reshape(4, 4, GROUP)
    groups = jnp.where(
        groups < 0, -1, groups // GROUP * SLOTS + groups % GROUP + 32 * jnp.arange(4, dtype=jnp.int32)[:, None, None]
    )
    slots = jnp.pad(groups, ((0, 0), (0, 0), (0, SLOTS - GROUP)), constant_values=-1).reshape(1, 128)
    gates = here(cache_gates)
    keys = here(cache_keys)
    values = here(cache_values)
    small = near_memory((8, 128), F32)
    normed, link, turned, offsets, last_part, bias, own_gain = kernel(
        prepare_kernel,
        (
            near_memory((128, 2048), BF16),
            near_memory((128, 128), F32),
            near_memory((128, 128), F32),
            near_memory((8, 128), jnp.int32),
            small,
            small,
            small,
        ),
        in_specs=[smem, smem] + [vmem] * 6,
        scratch_shapes=[pltpu.VMEM((128, 2048), F32)],
    )(
        lengths,
        accepted,
        tokens,
        norm_gain.reshape(1, -1),
        slots,
        forget_bias.reshape(8, 1),
        gates,
        head_gain.reshape(4, 128),
    )
    pieces, log_gate = kernel(
        project_kernel,
        (near_memory((16, 3, 8, 128), BF16), small),
        scratch_shapes=[pltpu.VMEM((32, 2048), F32)],
    )(here(columns), here(normed), here(bias))
    line = spread(pieces, KV[0])
    plane = here(spread(jnp.broadcast_to(line[None], (4, *line.shape)), KV[1]))

    partial, near, climb = kernel(
        attend_kernel,
        (near_memory((16, 4, 8, 128), BF16), near_memory((3, 8, 128), F32), small),
        scratch_shapes=[pltpu.VMEM((128, 512), F32)],
    )(
        here(offsets),
        here(last_part),
        plane,
        keys,
        values,
        gates,
        here(log_gate),
        here(link),
        here(turned),
    )
    received = spread(partial.reshape(64, 8, 128), KV)
    heads, last = kernel(merge_kernel, (near_memory((64, 8, 128), BF16), small))(
        here(received), here(near), here(own_gain)
    )
    everyone = spread(heads, KV)
    cache_spec = pl.BlockSpec((1, rows, 512), lambda b: (b, 0, 0))
    keys_out, values_out = kernel(
        write_kernel,
        (
            jax.ShapeDtypeStruct(cache_keys.shape, BF16),
            jax.ShapeDtypeStruct(cache_values.shape, BF16),
        ),
        grid=(4,),
        in_specs=[smem, smem, vmem, cache_spec, cache_spec],
        out_specs=(cache_spec, cache_spec),
    )(lengths, accepted, plane, cache_keys, cache_values)
    gates_out = kernel(gates_kernel, jax.ShapeDtypeStruct(cache_gates.shape, F32))(
        here(offsets), here(last), here(climb), gates
    )

    share = kernel(mix_kernel, near_memory((32, 128), F32))(here(everyone), here(w_out.T))
    shares = lax.all_gather(share, "tp")
    mixed = kernel(finish_kernel, jax.ShapeDtypeStruct((4, 32 // pair_count, 24), F32))(here(shares))
    mixed = jnp.swapaxes(mixed, 1, 2)
    return (mixed, keys_out, values_out, gates_out)


def solution(mesh):
    torus = Mesh(
        mesh.devices.reshape(mesh.shape["dp"], 16, 4, mesh.shape["tp"]),
        ("dp", "kv_0", "kv_1", "tp"),
    )
    return jax.shard_map(
        step,
        mesh=torus,
        in_specs=(
            P("dp", None, None),
            P(),
            P(KV, "tp"),
            P(KV, "tp"),
            P(KV, "tp"),
            P(KV, "tp"),
            P("tp"),
            P("tp"),
            P("tp", KV),
            P("dp", KV, "tp"),
            P("dp", KV, "tp"),
            P("dp", "tp", KV),
            P("dp"),
            P("dp"),
            P("dp", None),
        ),
        out_specs=(P("dp", None, KV_TP), P("dp", KV, "tp"), P("dp", KV, "tp"), P("dp", "tp", KV)),
        check_vma=False,
    )
```

```python
import jax
import jax.numpy as jnp
from jax import lax
from jax.experimental import pallas as pl
from jax.experimental.pallas import tpu as pltpu
from jax.sharding import Mesh
from jax.sharding import PartitionSpec as P


KV = ("kv_0", "kv_1")
KV_TP = ("kv_0", "kv_1", "tp")

NEG_LARGE = -1e30
EPSILON = 1e-06
F32 = jnp.float32
BF16 = jnp.bfloat16

GROUP = 6
SLOTS = 8
NT = (((1,), (1,)), ((), ()))
INTERPRET = False


def iota(shape, dim):
    return lax.broadcasted_iota(jnp.int32, shape, dim)


def three_parts(x):
    high = x.astype(BF16).astype(F32)
    rest = x - high
    middle = rest.astype(BF16).astype(F32)
    return high, middle, rest - middle


def merger(index):
    return index // 16, (index // 4) % 4, index % 4


def pack_kernel(wq_ref, wk_ref, wv_ref, wf_ref, out_ref):
    rows = wq_ref.shape[0]
    stacked = jnp.concatenate(
        [wq_ref[...].astype(F32), wk_ref[...].astype(F32), wv_ref[...].astype(F32), jnp.zeros((rows, wq_ref.shape[1]), F32)],
        axis=0,
    )
    turned = stacked.T
    queries = turned.reshape(16, 4, 8, 128)
    block = iota((128, 128), 1) // rows
    line = queries[:, 0].reshape(128, 128)
    for g in range(1, 4):
        line = jnp.where(block == g, pltpu.roll(queries[:, g].reshape(128, 128), g * rows, 1), line)
    line = jnp.broadcast_to(line.reshape(16, 1, 8, 128), (16, 4, 8, 128)).reshape(64, 8, 128)
    out_ref[:, 0] = line.astype(BF16)
    turned = turned.reshape(64, 8, 128)
    forget = jnp.concatenate([jnp.zeros((8, 3 * rows), F32), wf_ref[...].astype(F32)], axis=1)
    lane = iota((1, 8, 128), 2)
    out_ref[:, 1] = jnp.where(lane >= 3 * rows, forget[None], turned).astype(BF16)


def prepare_kernel(
    len_ref, acc_ref, tok_ref, gain_ref, par_ref, bias_ref, gate_ref, head_gain_ref,
    out_ref, link_ref, turned_ref, off_ref, last_ref, bias_out_ref, own_gain_ref, nrm_ref,
):
    rows = gate_ref.shape[2]
    index = lax.axis_index(KV)
    start = index * rows
    nrm_ref[...] = jnp.zeros(nrm_ref.shape, F32)
    gain = gain_ref[...].astype(F32)
    for b in range(4):
        tok = tok_ref[b].astype(F32)
        normed = tok * lax.rsqrt(jnp.mean(tok * tok, axis=1, keepdims=True) + EPSILON) * gain
        for g in range(4):
            at = b * 32 + g * SLOTS
            nrm_ref[at : at + GROUP, :] = normed[g * GROUP : (g + 1) * GROUP]
    out_ref[...] = nrm_ref[...].astype(BF16)

    child = iota((128, 128), 0)
    linked = ((par_ref[...] == child) | (child == iota((128, 128), 1))).astype(F32)
    for _ in range(5):
        low = linked.astype(BF16)
        linked = jnp.minimum(jnp.dot(low, low, preferred_element_type=F32), 1.0)
    link_ref[...] = linked
    turned_ref[...] = linked.T

    lane = iota((8, 128), 1)
    row = iota((8, 128), 0)
    total = jnp.zeros((8, 128), F32)
    offsets = jnp.zeros((8, 128), jnp.int32)
    for s in range(4):
        off = len_ref[s] + acc_ref[s] - start
        offsets = jnp.where(row == s, off, offsets)
        found = jnp.sum(jnp.where(iota((8, rows), 1) == off - 1, gate_ref[s], 0.0), axis=1, keepdims=True)
        high, middle, low = three_parts(jnp.broadcast_to(found, (8, 128)))
        value = jnp.where(lane < 32, high, jnp.where(lane < 64, middle, low))
        total = total + jnp.where((lane % 32 == s * 8 + row) & (lane < 96), value, 0.0)
    off_ref[...] = offsets
    last_ref[...] = jnp.broadcast_to(jnp.sum(total, axis=0, keepdims=True), (8, 128))
    bias_out_ref[...] = jnp.broadcast_to(bias_ref[...], (8, 128))
    own = jnp.where(iota((4, 128), 0) == merger(index)[0], head_gain_ref[...].astype(F32), 0.0)
    own_gain_ref[...] = jnp.broadcast_to(jnp.sum(own, axis=0, keepdims=True), (8, 128))


def project_kernel(x_ref, nrm_ref, bias_ref, piece_ref, gate_ref, wt_ref):
    block = iota((128, 128), 1) // 32
    tiles = [x_ref[:, k].astype(F32).reshape(16, 4, 8, 128) for k in range(2)]
    wanted = [(0, 0), (0, 1), (0, 2), (0, 3), (1, 1), (1, 2), (1, 3)]
    for at, (k, t) in enumerate(wanted):
        row = None
        for n in range(4):
            moved = tiles[k][:, n].reshape(128, 128)
            if n != t:
                moved = pltpu.roll(moved, ((n - t) * 32) % 128, 1)
            row = moved if row is None else jnp.where(block == n, moved, row)
        row = row.reshape(16, 8, 128)
        for m in range(16):
            wt_ref[at * 8 : (at + 1) * 8, m * 128 : (m + 1) * 128] = row[m]
    out = lax.dot_general(wt_ref[...].astype(BF16), nrm_ref[...], NT, preferred_element_type=F32)
    piece = out[:48].reshape(6, 8, 128).astype(BF16)
    piece_ref[...] = jnp.broadcast_to(piece[None], piece_ref.shape)
    pre = out[48:] + bias_ref[...]
    gate_ref[...] = jnp.minimum(pre, 0.0) - jnp.log1p(jnp.exp(-jnp.abs(pre)))


def slot_token(lane):
    return jnp.where(lane % SLOTS < GROUP, (lane % 32) // SLOTS * GROUP + lane % SLOTS, -100000)


def placement(b, off, rows):
    lane = iota((rows, 128), 1)
    return (iota((rows, 128), 0) - off == slot_token(lane)) & (lane // 32 == b)


def columns_of(g_ref, n, start, count):
    parts = [g_ref[y, pl.ds(start, count), n].astype(F32) for y in range(4)]
    return jnp.stack(parts, axis=1).reshape(count * 32, 128)


def attend_kernel(off_ref, last_ref, g_ref, k_ref, v_ref, gate_ref, out_ref, own_ref, query_ref, q_ref):
    rows = k_ref.shape[1]
    own_ref[...] = g_ref[:, 4:]
    q_ref[...] = g_ref[:, :4].astype(F32).reshape(512, 128).T * 0.125
    query_ref[...] = q_ref[...]
    half = iota((32, 128), 1) < 64
    lane = iota((64, 128), 1)
    row = iota((64, 128), 0)
    mine = (lane % 8 == row % 8) & ((lane // 64) == (row // 32))
    part = (iota((4, 8, 128), 2) % 64) // 8
    slot = iota((4, 8, 128), 1)
    last = last_ref[...][None]

    def scores_of(b):
        found = []
        for p in range(4):
            q = q_ref[b * 32 : (b + 1) * 32, p * 128 : (p + 1) * 128]
            both = jnp.concatenate([jnp.where(half, q, 0.0), jnp.where(half, 0.0, q)], axis=0).astype(BF16)
            found.append(
                lax.dot_general(both, k_ref[b, :, p * 128 : (p + 1) * 128], NT, preferred_element_type=F32)
            )
        return found

    ahead = scores_of(0)
    for b in range(4):
        scores, ahead = ahead, scores_of(b + 1) if b < 3 else None
        off = off_ref[b : b + 1, 0:1]
        gates = jnp.where(iota((8, rows), 1) < off, gate_ref[b], -NEG_LARGE)
        for p in range(4):
            shifts = [jnp.broadcast_to(gates[2 * p + k : 2 * p + k + 1], (32, rows)) for k in range(2)]
            shifted = scores[p] - jnp.concatenate(shifts, axis=0)
            highest = jnp.max(shifted, axis=1, keepdims=True)
            weights = jnp.exp(shifted - highest)
            total = jnp.sum(weights, axis=1, keepdims=True)
            weighted = jnp.dot(
                weights.astype(BF16), v_ref[b, :, p * 128 : (p + 1) * 128], preferred_element_type=F32
            )
            weighted = weighted * (1.0 / total)
            level = jnp.where(mine, highest + jnp.log(total), 0.0)
            level = jnp.sum((level[:32] + level[32:]).reshape(4, 8, 128), axis=1, keepdims=True)
            level = jnp.broadcast_to(jnp.where(off > 0, level, NEG_LARGE), (4, 8, 128))
            high, middle, low = three_parts(level)
            level = jnp.where(part == 0, high, jnp.where(part == 1, middle, low))
            pair = jnp.where(half, weighted[:32], weighted[32:]).reshape(4, 8, 128)
            pair = jnp.where(slot == 6, level, jnp.where(slot == 7, last, pair))
            out_ref[p * 4 : (p + 1) * 4, b] = pair.astype(BF16)


def near_kernel(g_ref, q_ref, lg_ref, link_ref, turned_ref, near_ref, climb_ref):
    parts = jnp.concatenate(three_parts(lg_ref[...]), axis=0).astype(BF16)
    summed = jnp.dot(parts, link_ref[...].astype(BF16), preferred_element_type=F32)
    climb = summed[:8] + summed[8:16] + summed[16:]
    climb_ref[...] = climb
    p, group, seq = merger(lax.axis_index(KV))
    half = iota((8, 128), 1) < 64
    at = pl.multiple_of(seq * 32 + group * 8, 8)
    keys = columns_of(g_ref, 0, p * 4, 4).astype(BF16)
    values = columns_of(g_ref, 1, p * 4, 4).astype(BF16)
    q = q_ref[pl.ds(at, 8), pl.ds(pl.multiple_of(p * 128, 128), 128)]
    both = jnp.concatenate([jnp.where(half, q, 0.0), jnp.where(half, 0.0, q)], axis=0).astype(BF16)
    near = jnp.dot(both, keys, preferred_element_type=F32)
    head = iota((8, 128), 0)
    climbs = [jnp.sum(jnp.where(head == 2 * p + k, climb, 0.0), axis=0, keepdims=True) for k in range(2)]
    near = near - jnp.concatenate([jnp.broadcast_to(c, (8, 128)) for c in climbs], axis=0)
    linked = turned_ref[pl.ds(at, 8), :]
    linked = jnp.concatenate([linked, linked], axis=0) > 0.5
    near = jnp.where(linked, near, NEG_LARGE)
    near_top = jnp.max(near, axis=1, keepdims=True)
    near = jnp.where(linked, jnp.exp(near - near_top), 0.0)
    near_sum = jnp.sum(near, axis=1, keepdims=True)
    near = lax.dot_general(near.astype(BF16), values, NT, preferred_element_type=F32)
    near_ref[0] = jnp.where(half, near[:8], near[8:])
    near_ref[1] = jnp.where(half, near_top[:8], near_top[8:])
    near_ref[2] = jnp.where(half, near_sum[:8], near_sum[8:])


def write_kernel(len_ref, acc_ref, g_ref, k_ref, v_ref, kout_ref, vout_ref):
    b = pl.program_id(0)
    rows = k_ref.shape[1]
    off = len_ref[b] + acc_ref[b] - lax.axis_index(KV) * rows
    landing = (off > -24) & (off < rows)

    @pl.when(jnp.logical_not(landing))
    def _():
        kout_ref[...] = k_ref[...]
        vout_ref[...] = v_ref[...]

    @pl.when(landing)
    def _():
        placed = placement(b, off, rows).astype(F32).astype(BF16)
        index = iota((rows, 512), 0)
        landed = (index >= off) & (index < off + 24)
        for n, source, target in ((0, k_ref, kout_ref), (1, v_ref, vout_ref)):
            fresh = columns_of(g_ref, n, 0, 16).astype(BF16)
            written = lax.dot_general(placed, fresh, NT, preferred_element_type=F32)
            target[0] = jnp.where(landed, written, source[0].astype(F32)).astype(BF16)


def merge_kernel(r_ref, near_ref, gain_ref, out_ref, last_ref):
    p, _, seq = merger(lax.axis_index(KV))
    got = r_ref[...].astype(F32)
    lane3 = iota((64, 8, 128), 2)
    keep = (lane3 % 8 == iota((64, 8, 128), 1)) & ((lane3 % 64) // 8 < 3)
    level = jnp.where(keep, got[:, 6:7, :], 0.0).reshape(512, 128).astype(BF16)
    halves = (iota((128, 128), 0) // 64 == iota((128, 128), 1) // 64).astype(F32).astype(BF16)
    level = jnp.dot(level, halves, preferred_element_type=F32).reshape(64, 8, 128)
    top = jnp.max(level, axis=0)
    scale = jnp.exp(level - top[None])
    far_sum = jnp.sum(scale, axis=0)
    far = jnp.sum(scale * got, axis=0)
    whole = jnp.sum(got, axis=0)
    last_ref[...] = whole
    last = whole[7:8]

    half = iota((8, 128), 1) < 64
    lane1 = iota((1, 128), 1)
    first = seq * 8 + 2 * p
    pick = [
        jnp.sum(jnp.where((lane1 % 32 == first + k) & (lane1 < 96), last, 0.0), axis=1, keepdims=True)
        for k in range(2)
    ]
    top = top + jnp.where(half, pick[0], pick[1])
    near, near_top, near_sum = near_ref[0], near_ref[1], near_ref[2]
    overall = jnp.maximum(top, near_top)
    far_scale = jnp.exp(top - overall)
    near_scale = jnp.exp(near_top - overall)
    attended = (far * far_scale + near * near_scale) / (far_sum * far_scale + near_sum * near_scale)
    square = attended * attended
    low = jnp.sum(jnp.where(half, square, 0.0), axis=1, keepdims=True)
    high = jnp.sum(jnp.where(half, 0.0, square), axis=1, keepdims=True)
    mean = jnp.where(half, low, high) * (1.0 / 64.0)
    heads = (attended * lax.rsqrt(mean + EPSILON) * gain_ref[...]).astype(BF16)
    out_ref[...] = jnp.broadcast_to(heads[None], out_ref.shape)


def gates_kernel(off_ref, last_ref, climb_ref, gate_ref, gout_ref):
    rows = gate_ref.shape[2]
    last = last_ref[...][7:8]
    lane = iota((32, 128), 1)
    column = jnp.sum(jnp.where((lane % 32 == iota((32, 128), 0)) & (lane < 96), last, 0.0), axis=1, keepdims=True)
    parts = jnp.concatenate(three_parts(climb_ref[...]), axis=0).astype(BF16)
    for b in range(4):
        off = off_ref[b : b + 1, 0:1]
        placed = placement(b, off, rows).astype(F32).astype(BF16)
        written = lax.dot_general(parts, placed, NT, preferred_element_type=F32)
        written = written[:8] + written[8:16] + written[16:] + column[b * 8 : (b + 1) * 8]
        spot = iota((8, rows), 1)
        gout_ref[b] = jnp.where((spot >= off) & (spot < off + 24), written, gate_ref[b])


def mix_kernel(g_ref, w_ref, out_ref):
    total = jnp.zeros((32, 128), F32)
    for p in range(4):
        heads = g_ref[p * 16 : (p + 1) * 16].astype(F32).reshape(128, 128).astype(BF16)
        total = total + lax.dot_general(w_ref[:, p * 128 : (p + 1) * 128], heads, NT, preferred_element_type=F32)
    out_ref[...] = total.reshape(out_ref.shape)


def finish_kernel(x_ref, out_ref):
    width = out_ref.shape[1]
    own = pl.multiple_of(lax.axis_index("tp") * width, width)
    total = x_ref[0, pl.ds(own, width), :]
    for k in range(1, x_ref.shape[0]):
        total = total + x_ref[k, pl.ds(own, width), :]
    for g in range(4):
        for b in range(4):
            at = (g * 4 + b) * SLOTS
            out_ref[b, :, g * GROUP : (g + 1) * GROUP] = total[:, at : at + GROUP]


GRANTS = {project_kernel: 16 * 2**20, attend_kernel: 16 * 2**20}


def spread(array, axis):
    return lax.all_to_all(array, axis, split_axis=0, concat_axis=0, tiled=True)


def near_memory(shape, dtype):
    return pltpu.VMEM(shape, dtype)


def here(array):
    return pltpu.with_memory_space_constraint(array, pltpu.VMEM)


def step(
    tokens,
    norm_gain,
    w_query,
    w_key,
    w_value,
    w_forget,
    forget_bias,
    head_gain,
    w_out,
    cache_keys,
    cache_values,
    cache_gates,
    lengths,
    accepted,
    parents,
):
    rows = cache_keys.shape[1]
    pair_count = lax.axis_size("tp")
    smem = pl.BlockSpec(memory_space=pltpu.SMEM)
    vmem = pl.BlockSpec(memory_space=pltpu.VMEM)

    def kernel(body, out_shape, **kw):
        params = pltpu.CompilerParams(vmem_limit_bytes=GRANTS.get(body))
        return pl.pallas_call(body, out_shape=out_shape, interpret=INTERPRET, compiler_params=params, **kw)

    packed = kernel(pack_kernel, near_memory((64, 2, 8, 128), BF16))(w_query, w_key, w_value, w_forget.T)
    columns = spread(packed, KV)

    groups = parents.reshape(4, 4, GROUP)
    groups = jnp.where(
        groups < 0, -1, groups // GROUP * SLOTS + groups % GROUP + 32 * jnp.arange(4, dtype=jnp.int32)[:, None, None]
    )
    slots = jnp.pad(groups, ((0, 0), (0, 0), (0, SLOTS - GROUP)), constant_values=-1).reshape(1, 128)
    gates = here(cache_gates)
    keys = here(cache_keys)
    values = here(cache_values)
    small = near_memory((8, 128), F32)
    normed, link, turned, offsets, last_part, bias, own_gain = kernel(
        prepare_kernel,
        (
            near_memory((128, 2048), BF16),
            near_memory((128, 128), F32),
            near_memory((128, 128), F32),
            near_memory((8, 128), jnp.int32),
            small,
            small,
            small,
        ),
        in_specs=[smem, smem] + [vmem] * 6,
        scratch_shapes=[pltpu.VMEM((128, 2048), F32)],
    )(
        lengths,
        accepted,
        tokens,
        norm_gain.reshape(1, -1),
        slots,
        forget_bias.reshape(8, 1),
        gates,
        head_gain.reshape(4, 128),
    )
    pieces, log_gate = kernel(
        project_kernel,
        (near_memory((16, 6, 8, 128), BF16), small),
        scratch_shapes=[pltpu.VMEM((56, 2048), F32)],
    )(here(columns), here(normed), here(bias))
    line = spread(pieces, KV[0])
    partial, own, query = kernel(
        attend_kernel,
        (near_memory((16, 4, 8, 128), BF16), near_memory((16, 2, 8, 128), BF16), near_memory((128, 512), F32)),
        scratch_shapes=[pltpu.VMEM((128, 512), F32)],
    )(here(offsets), here(last_part), here(line), keys, values, gates)
    received = spread(partial.reshape(64, 8, 128), KV)
    two = lax.all_gather(own, KV[1], axis_index_groups=[[0, 1], [2, 3]])
    plane = lax.all_gather(two, KV[1], axis_index_groups=[[0, 3], [1, 2]])
    plane = here(plane.reshape(4, *own.shape))
    near, climb = kernel(near_kernel, (near_memory((3, 8, 128), F32), small))(
        plane, here(query), here(log_gate), here(link), here(turned)
    )
    heads, last = kernel(merge_kernel, (near_memory((64, 8, 128), BF16), small))(
        here(received), here(near), here(own_gain)
    )
    everyone = spread(heads, KV)
    cache_spec = pl.BlockSpec((1, rows, 512), lambda b: (b, 0, 0))
    keys_out, values_out = kernel(
        write_kernel,
        (
            jax.ShapeDtypeStruct(cache_keys.shape, BF16),
            jax.ShapeDtypeStruct(cache_values.shape, BF16),
        ),
        grid=(4,),
        in_specs=[smem, smem, vmem, cache_spec, cache_spec],
        out_specs=(cache_spec, cache_spec),
    )(lengths, accepted, plane, cache_keys, cache_values)
    gates_out = kernel(gates_kernel, jax.ShapeDtypeStruct(cache_gates.shape, F32))(
        here(offsets), here(last), here(climb), gates
    )

    share = kernel(mix_kernel, near_memory((32, 128), F32))(here(everyone), here(w_out.T))
    shares = lax.all_gather(share, "tp")
    mixed = kernel(finish_kernel, jax.ShapeDtypeStruct((4, 32 // pair_count, 24), F32))(here(shares))
    mixed = jnp.swapaxes(mixed, 1, 2)
    return (mixed, keys_out, values_out, gates_out)


def solution(mesh):
    torus = Mesh(
        mesh.devices.reshape(mesh.shape["dp"], 16, 4, mesh.shape["tp"]),
        ("dp", "kv_0", "kv_1", "tp"),
    )
    return jax.shard_map(
        step,
        mesh=torus,
        in_specs=(
            P("dp", None, None),
            P(),
            P(KV, "tp"),
            P(KV, "tp"),
            P(KV, "tp"),
            P(KV, "tp"),
            P("tp"),
            P("tp"),
            P("tp", KV),
            P("dp", KV, "tp"),
            P("dp", KV, "tp"),
            P("dp", "tp", KV),
            P("dp"),
            P("dp"),
            P("dp", None),
        ),
        out_specs=(P("dp", None, KV_TP), P("dp", KV, "tp"), P("dp", KV, "tp"), P("dp", "tp", KV)),
        check_vma=False,
    )
```

```python
import jax
import jax.numpy as jnp
from jax import lax
from jax.experimental import pallas as pl
from jax.experimental.pallas import tpu as pltpu
from jax.sharding import Mesh
from jax.sharding import PartitionSpec as P


KV = "kv"
KV_TP = ("kv", "tp")

LINE, PLANE = 16, 4
FIRST = (9, 2)
MEMBERS = [(z + FIRST[0]) % LINE * PLANE + (y + FIRST[1]) % PLANE for z in range(LINE) for y in range(PLANE)]
ALL = [MEMBERS]
LINES = [MEMBERS[y::PLANE] for y in range(PLANE)]
PLANES = [MEMBERS[z * PLANE : (z + 1) * PLANE] for z in range(LINE)]

NEG_LARGE = -1e30
EPSILON = 1e-06
F32 = jnp.float32
BF16 = jnp.bfloat16

GROUP = 6
SLOTS = 8
NT = (((1,), (1,)), ((), ()))
INTERPRET = False


def iota(shape, dim):
    return lax.broadcasted_iota(jnp.int32, shape, dim)


def three_parts(x):
    high = x.astype(BF16).astype(F32)
    rest = x - high
    middle = rest.astype(BF16).astype(F32)
    return high, middle, rest - middle


def merger(index):
    z = (index // PLANE + LINE - FIRST[0]) % LINE
    return z // 4, z % 4, (index + PLANE - FIRST[1]) % PLANE


def pack_kernel(wq_ref, wk_ref, wv_ref, wf_ref, out_ref):
    rows = wq_ref.shape[0]
    stacked = jnp.concatenate(
        [wq_ref[...].astype(F32), wk_ref[...].astype(F32), wv_ref[...].astype(F32), jnp.zeros((rows, wq_ref.shape[1]), F32)],
        axis=0,
    )
    turned = stacked.T.reshape(out_ref.shape)
    forget = jnp.concatenate([jnp.zeros((8, 3 * rows), F32), wf_ref[...].astype(F32)], axis=1)
    lane = iota((1, 8, 128), 2)
    out_ref[...] = jnp.where(lane >= 3 * rows, forget[None], turned).astype(BF16)


def prepare_kernel(
    len_ref, acc_ref, tok_ref, gain_ref, par_ref, bias_ref, gate_ref, head_gain_ref,
    out_ref, link_ref, turned_ref, off_ref, last_ref, bias_out_ref, own_gain_ref, nrm_ref,
):
    rows = gate_ref.shape[2]
    index = lax.axis_index(KV)
    start = index * rows
    nrm_ref[...] = jnp.zeros(nrm_ref.shape, F32)
    gain = gain_ref[...].astype(F32)
    for b in range(4):
        tok = tok_ref[b].astype(F32)
        normed = tok * lax.rsqrt(jnp.mean(tok * tok, axis=1, keepdims=True) + EPSILON) * gain
        for g in range(4):
            at = b * 32 + g * SLOTS
            nrm_ref[at : at + GROUP, :] = normed[g * GROUP : (g + 1) * GROUP]
    for z in range(LINE):
        at = (z + FIRST[0]) % LINE * 128
        features = pltpu.roll(nrm_ref[:, at : at + 128], (PLANE - FIRST[1]) % PLANE * 32, 1)
        out_ref[:, z * 128 : (z + 1) * 128] = features.astype(BF16)

    child = iota((128, 128), 0)
    linked = ((par_ref[...] == child) | (child == iota((128, 128), 1))).astype(F32)
    for _ in range(5):
        low = linked.astype(BF16)
        linked = jnp.minimum(jnp.dot(low, low, preferred_element_type=F32), 1.0)
    link_ref[...] = linked
    turned_ref[...] = linked.T

    lane = iota((8, 128), 1)
    row = iota((8, 128), 0)
    total = jnp.zeros((8, 128), F32)
    offsets = jnp.zeros((8, 128), jnp.int32)
    for s in range(4):
        off = len_ref[s] + acc_ref[s] - start
        offsets = jnp.where(row == s, off, offsets)
        found = jnp.sum(jnp.where(iota((8, rows), 1) == off - 1, gate_ref[s], 0.0), axis=1, keepdims=True)
        high, middle, low = three_parts(jnp.broadcast_to(found, (8, 128)))
        value = jnp.where(lane < 32, high, jnp.where(lane < 64, middle, low))
        total = total + jnp.where((lane % 32 == s * 8 + row) & (lane < 96), value, 0.0)
    off_ref[...] = offsets
    last_ref[...] = jnp.broadcast_to(jnp.sum(total, axis=0, keepdims=True), (8, 128))
    bias_out_ref[...] = jnp.broadcast_to(bias_ref[...], (8, 128))
    own = jnp.where(iota((4, 128), 0) == merger(index)[0], head_gain_ref[...].astype(F32), 0.0)
    own_gain_ref[...] = jnp.broadcast_to(jnp.sum(own, axis=0, keepdims=True), (8, 128))


def project_kernel(x_ref, nrm_ref, bias_ref, piece_ref, gate_ref, wt_ref):
    x = x_ref[...].astype(F32).reshape(16, 4, 8, 128)
    block = iota((128, 128), 1) // 32
    for t in range(4):
        row = None
        for n in range(4):
            moved = x[:, n].reshape(128, 128)
            if n != t:
                moved = pltpu.roll(moved, ((n - t) * 32) % 128, 1)
            row = moved if row is None else jnp.where(block == n, moved, row)
        row = row.reshape(16, 8, 128)
        for m in range(16):
            wt_ref[t * 8 : (t + 1) * 8, m * 128 : (m + 1) * 128] = row[m]
    out = lax.dot_general(wt_ref[...].astype(BF16), nrm_ref[...], NT, preferred_element_type=F32)
    piece = out[:24].reshape(3, 8, 128).astype(BF16)
    piece_ref[...] = jnp.broadcast_to(piece[None], piece_ref.shape)
    pre = out[24:] + bias_ref[...]
    gate_ref[...] = jnp.minimum(pre, 0.0) - jnp.log1p(jnp.exp(-jnp.abs(pre)))


def slot_token(lane):
    return jnp.where(lane % SLOTS < GROUP, (lane % 32) // SLOTS * GROUP + lane % SLOTS, -100000)


def placement(b, off, rows):
    lane = iota((rows, 128), 1)
    return (iota((rows, 128), 0) - off == slot_token(lane)) & (lane // 32 == b)


def columns_of(g_ref, n, start, count):
    parts = [g_ref[y, pl.ds(start, count), n].astype(F32) for y in range(4)]
    return jnp.stack(parts, axis=1).reshape(count * 32, 128)


def attend_kernel(
    off_ref, last_ref, g_ref, k_ref, v_ref, gate_ref, lg_ref, link_ref, turned_ref,
    out_ref, near_ref, climb_ref, q_ref,
):
    rows = k_ref.shape[1]
    q_ref[...] = columns_of(g_ref, 0, 0, 16).T * 0.125
    half = iota((32, 128), 1) < 64
    lane = iota((64, 128), 1)
    row = iota((64, 128), 0)
    mine = (lane % 8 == row % 8) & ((lane // 64) == (row // 32))
    part = (iota((4, 8, 128), 2) % 64) // 8
    slot = iota((4, 8, 128), 1)
    last = last_ref[...][None]

    def scores_of(b):
        found = []
        for p in range(4):
            q = q_ref[b * 32 : (b + 1) * 32, p * 128 : (p + 1) * 128]
            both = jnp.concatenate([jnp.where(half, q, 0.0), jnp.where(half, 0.0, q)], axis=0).astype(BF16)
            found.append(
                lax.dot_general(both, k_ref[b, :, p * 128 : (p + 1) * 128], NT, preferred_element_type=F32)
            )
        return found

    ahead = scores_of(0)
    for b in range(4):
        scores, ahead = ahead, scores_of(b + 1) if b < 3 else None
        off = off_ref[b : b + 1, 0:1]
        gates = jnp.where(iota((8, rows), 1) < off, gate_ref[b], -NEG_LARGE)
        for p in range(4):
            shifts = [jnp.broadcast_to(gates[2 * p + k : 2 * p + k + 1], (32, rows)) for k in range(2)]
            shifted = scores[p] - jnp.concatenate(shifts, axis=0)
            highest = jnp.max(shifted, axis=1, keepdims=True)
            weights = jnp.exp(shifted - highest)
            total = jnp.sum(weights, axis=1, keepdims=True)
            weighted = jnp.dot(
                weights.astype(BF16), v_ref[b, :, p * 128 : (p + 1) * 128], preferred_element_type=F32
            )
            weighted = weighted * (1.0 / total)
            level = jnp.where(mine, highest + jnp.log(total), 0.0)
            level = jnp.sum((level[:32] + level[32:]).reshape(4, 8, 128), axis=1, keepdims=True)
            level = jnp.broadcast_to(jnp.where(off > 0, level, NEG_LARGE), (4, 8, 128))
            high, middle, low = three_parts(level)
            level = jnp.where(part == 0, high, jnp.where(part == 1, middle, low))
            pair = jnp.where(half, weighted[:32], weighted[32:]).reshape(4, 8, 128)
            pair = jnp.where(slot == 6, level, jnp.where(slot == 7, last, pair))
            out_ref[p * 4 : (p + 1) * 4, b] = pair.astype(BF16)

    parts = jnp.concatenate(three_parts(lg_ref[...]), axis=0).astype(BF16)
    summed = jnp.dot(parts, link_ref[...].astype(BF16), preferred_element_type=F32)
    climb = summed[:8] + summed[8:16] + summed[16:]
    climb_ref[...] = climb
    p, group, seq = merger(lax.axis_index(KV))
    half = iota((8, 128), 1) < 64
    at = pl.multiple_of(seq * 32 + group * 8, 8)
    keys = columns_of(g_ref, 1, p * 4, 4).astype(BF16)
    values = columns_of(g_ref, 2, p * 4, 4).astype(BF16)
    q = q_ref[pl.ds(at, 8), pl.ds(pl.multiple_of(p * 128, 128), 128)]
    both = jnp.concatenate([jnp.where(half, q, 0.0), jnp.where(half, 0.0, q)], axis=0).astype(BF16)
    near = jnp.dot(both, keys, preferred_element_type=F32)
    head = iota((8, 128), 0)
    climbs = [jnp.sum(jnp.where(head == 2 * p + k, climb, 0.0), axis=0, keepdims=True) for k in range(2)]
    near = near - jnp.concatenate([jnp.broadcast_to(c, (8, 128)) for c in climbs], axis=0)
    linked = turned_ref[pl.ds(at, 8), :]
    linked = jnp.concatenate([linked, linked], axis=0) > 0.5
    near = jnp.where(linked, near, NEG_LARGE)
    near_top = jnp.max(near, axis=1, keepdims=True)
    near = jnp.where(linked, jnp.exp(near - near_top), 0.0)
    near_sum = jnp.sum(near, axis=1, keepdims=True)
    near = lax.dot_general(near.astype(BF16), values, NT, preferred_element_type=F32)
    near_ref[0] = jnp.where(half, near[:8], near[8:])
    near_ref[1] = jnp.where(half, near_top[:8], near_top[8:])
    near_ref[2] = jnp.where(half, near_sum[:8], near_sum[8:])


def write_kernel(len_ref, acc_ref, g_ref, k_ref, v_ref, kout_ref, vout_ref):
    b = pl.program_id(0)
    rows = k_ref.shape[1]
    off = len_ref[b] + acc_ref[b] - lax.axis_index(KV) * rows
    landing = (off > -24) & (off < rows)

    @pl.when(jnp.logical_not(landing))
    def _():
        kout_ref[...] = k_ref[...]
        vout_ref[...] = v_ref[...]

    @pl.when(landing)
    def _():
        placed = placement(b, off, rows).astype(F32).astype(BF16)
        index = iota((rows, 512), 0)
        landed = (index >= off) & (index < off + 24)
        for n, source, target in ((1, k_ref, kout_ref), (2, v_ref, vout_ref)):
            fresh = columns_of(g_ref, n, 0, 16).astype(BF16)
            written = lax.dot_general(placed, fresh, NT, preferred_element_type=F32)
            target[0] = jnp.where(landed, written, source[0].astype(F32)).astype(BF16)


def merge_kernel(r_ref, near_ref, gain_ref, out_ref, last_ref):
    p, _, seq = merger(lax.axis_index(KV))
    got = r_ref[...].astype(F32)
    lane3 = iota((64, 8, 128), 2)
    keep = (lane3 % 8 == iota((64, 8, 128), 1)) & ((lane3 % 64) // 8 < 3)
    level = jnp.where(keep, got[:, 6:7, :], 0.0).reshape(512, 128).astype(BF16)
    halves = (iota((128, 128), 0) // 64 == iota((128, 128), 1) // 64).astype(F32).astype(BF16)
    level = jnp.dot(level, halves, preferred_element_type=F32).reshape(64, 8, 128)
    top = jnp.max(level, axis=0)
    scale = jnp.exp(level - top[None])
    far_sum = jnp.sum(scale, axis=0)
    far = jnp.sum(scale * got, axis=0)
    whole = jnp.sum(got, axis=0)
    last_ref[...] = whole
    last = whole[7:8]

    half = iota((8, 128), 1) < 64
    lane1 = iota((1, 128), 1)
    first = seq * 8 + 2 * p
    pick = [
        jnp.sum(jnp.where((lane1 % 32 == first + k) & (lane1 < 96), last, 0.0), axis=1, keepdims=True)
        for k in range(2)
    ]
    top = top + jnp.where(half, pick[0], pick[1])
    near, near_top, near_sum = near_ref[0], near_ref[1], near_ref[2]
    overall = jnp.maximum(top, near_top)
    far_scale = jnp.exp(top - overall)
    near_scale = jnp.exp(near_top - overall)
    attended = (far * far_scale + near * near_scale) / (far_sum * far_scale + near_sum * near_scale)
    square = attended * attended
    low = jnp.sum(jnp.where(half, square, 0.0), axis=1, keepdims=True)
    high = jnp.sum(jnp.where(half, 0.0, square), axis=1, keepdims=True)
    mean = jnp.where(half, low, high) * (1.0 / 64.0)
    heads = (attended * lax.rsqrt(mean + EPSILON) * gain_ref[...]).astype(BF16)
    out_ref[...] = jnp.broadcast_to(heads[None], out_ref.shape)


def gates_kernel(off_ref, last_ref, climb_ref, gate_ref, gout_ref):
    rows = gate_ref.shape[2]
    last = last_ref[...][7:8]
    lane = iota((32, 128), 1)
    column = jnp.sum(jnp.where((lane % 32 == iota((32, 128), 0)) & (lane < 96), last, 0.0), axis=1, keepdims=True)
    parts = jnp.concatenate(three_parts(climb_ref[...]), axis=0).astype(BF16)
    for b in range(4):
        off = off_ref[b : b + 1, 0:1]
        placed = placement(b, off, rows).astype(F32).astype(BF16)
        written = lax.dot_general(parts, placed, NT, preferred_element_type=F32)
        written = written[:8] + written[8:16] + written[16:] + column[b * 8 : (b + 1) * 8]
        spot = iota((8, rows), 1)
        gout_ref[b] = jnp.where((spot >= off) & (spot < off + 24), written, gate_ref[b])


def mix_kernel(g_ref, w_ref, out_ref):
    total = jnp.zeros((32, 128), F32)
    for p in range(4):
        heads = g_ref[p * 16 : (p + 1) * 16].astype(F32).reshape(128, 128).astype(BF16)
        total = total + lax.dot_general(w_ref[:, p * 128 : (p + 1) * 128], heads, NT, preferred_element_type=F32)
    out_ref[...] = total.reshape(out_ref.shape)


def finish_kernel(x_ref, out_ref):
    width = out_ref.shape[1]
    own = pl.multiple_of(lax.axis_index("tp") * width, width)
    total = x_ref[0, pl.ds(own, width), :]
    for k in range(1, x_ref.shape[0]):
        total = total + x_ref[k, pl.ds(own, width), :]
    for g in range(4):
        for b in range(4):
            at = (g * 4 + b) * SLOTS
            out_ref[b, :, g * GROUP : (g + 1) * GROUP] = total[:, at : at + GROUP]


def spread(array, groups):
    return lax.all_to_all(array, KV, split_axis=0, concat_axis=0, tiled=True, axis_index_groups=groups)


def near_memory(shape, dtype):
    return pltpu.VMEM(shape, dtype)


def here(array):
    return pltpu.with_memory_space_constraint(array, pltpu.VMEM)


def step(
    tokens,
    norm_gain,
    w_query,
    w_key,
    w_value,
    w_forget,
    forget_bias,
    head_gain,
    w_out,
    cache_keys,
    cache_values,
    cache_gates,
    lengths,
    accepted,
    parents,
):
    rows = cache_keys.shape[1]
    pair_count = lax.axis_size("tp")
    smem = pl.BlockSpec(memory_space=pltpu.SMEM)
    vmem = pl.BlockSpec(memory_space=pltpu.VMEM)

    def kernel(body, out_shape, **kw):
        return pl.pallas_call(body, out_shape=out_shape, interpret=INTERPRET, **kw)

    packed = kernel(pack_kernel, near_memory((64, 8, 128), BF16))(w_query, w_key, w_value, w_forget.T)
    columns = spread(packed, ALL)

    groups = parents.reshape(4, 4, GROUP)
    groups = jnp.where(
        groups < 0, -1, groups // GROUP * SLOTS + groups % GROUP + 32 * jnp.arange(4, dtype=jnp.int32)[:, None, None]
    )
    slots = jnp.pad(groups, ((0, 0), (0, 0), (0, SLOTS - GROUP)), constant_values=-1).reshape(1, 128)
    gates = here(cache_gates)
    keys = here(cache_keys)
    values = here(cache_values)
    small = near_memory((8, 128), F32)
    normed, link, turned, offsets, last_part, bias, own_gain = kernel(
        prepare_kernel,
        (
            near_memory((128, 2048), BF16),
            near_memory((128, 128), F32),
            near_memory((128, 128), F32),
            near_memory((8, 128), jnp.int32),
            small,
            small,
            small,
        ),
        in_specs=[smem, smem] + [vmem] * 6,
        scratch_shapes=[pltpu.VMEM((128, 2048), F32)],
    )(
        lengths,
        accepted,
        tokens,
        norm_gain.reshape(1, -1),
        slots,
        forget_bias.reshape(8, 1),
        gates,
        head_gain.reshape(4, 128),
    )
    pieces, log_gate = kernel(
        project_kernel,
        (near_memory((16, 3, 8, 128), BF16), small),
        scratch_shapes=[pltpu.VMEM((32, 2048), F32)],
    )(here(columns), here(normed), here(bias))
    line = spread(pieces, LINES)
    plane = here(spread(jnp.broadcast_to(line[None], (4, *line.shape)), PLANES))

    partial, near, climb = kernel(
        attend_kernel,
        (near_memory((16, 4, 8, 128), BF16), near_memory((3, 8, 128), F32), small),
        scratch_shapes=[pltpu.VMEM((128, 512), F32)],
    )(
        here(offsets),
        here(last_part),
        plane,
        keys,
        values,
        gates,
        here(log_gate),
        here(link),
        here(turned),
    )
    received = spread(partial.reshape(64, 8, 128), ALL)
    heads, last = kernel(merge_kernel, (near_memory((64, 8, 128), BF16), small))(
        here(received), here(near), here(own_gain)
    )
    everyone = spread(heads, ALL)
    cache_spec = pl.BlockSpec((1, rows, 512), lambda b: (b, 0, 0))
    keys_out, values_out = kernel(
        write_kernel,
        (
            jax.ShapeDtypeStruct(cache_keys.shape, BF16),
            jax.ShapeDtypeStruct(cache_values.shape, BF16),
        ),
        grid=(4,),
        in_specs=[smem, smem, vmem, cache_spec, cache_spec],
        out_specs=(cache_spec, cache_spec),
    )(lengths, accepted, plane, cache_keys, cache_values)
    gates_out = kernel(gates_kernel, jax.ShapeDtypeStruct(cache_gates.shape, F32))(
        here(offsets), here(last), here(climb), gates
    )

    share = kernel(mix_kernel, near_memory((32, 128), F32))(here(everyone), here(w_out.T))
    shares = lax.all_gather(share, "tp")
    mixed = kernel(finish_kernel, jax.ShapeDtypeStruct((4, 32 // pair_count, 24), F32))(here(shares))
    mixed = jnp.swapaxes(mixed, 1, 2)
    return (mixed, keys_out, values_out, gates_out)


def solution(mesh):
    torus = Mesh(
        mesh.devices.reshape(mesh.shape["dp"], LINE * PLANE, mesh.shape["tp"]),
        ("dp", "kv", "tp"),
    )
    return jax.shard_map(
        step,
        mesh=torus,
        in_specs=(
            P("dp", None, None),
            P(),
            P(KV, "tp"),
            P(KV, "tp"),
            P(KV, "tp"),
            P(KV, "tp"),
            P("tp"),
            P("tp"),
            P("tp", KV),
            P("dp", KV, "tp"),
            P("dp", KV, "tp"),
            P("dp", "tp", KV),
            P("dp"),
            P("dp"),
            P("dp", None),
        ),
        out_specs=(P("dp", None, KV_TP), P("dp", KV, "tp"), P("dp", KV, "tp"), P("dp", "tp", KV)),
        check_vma=False,
    )
```

```python
import jax
import jax.numpy as jnp
from jax import lax
from jax.experimental import pallas as pl
from jax.experimental.pallas import tpu as pltpu
from jax.sharding import Mesh
from jax.sharding import PartitionSpec as P


KV = "kv"
KV_TP = ("kv", "tp")

LINE, PLANE = 16, 4
FIRST = (11, 2)
MEMBERS = [(z + FIRST[0]) % LINE * PLANE + (y + FIRST[1]) % PLANE for z in range(LINE) for y in range(PLANE)]
ALL = [MEMBERS]
LINES = [MEMBERS[y::PLANE] for y in range(PLANE)]
PLANES = [MEMBERS[z * PLANE : (z + 1) * PLANE] for z in range(LINE)]

NEG_LARGE = -1e30
EPSILON = 1e-06
F32 = jnp.float32
BF16 = jnp.bfloat16

GROUP = 6
SLOTS = 8
NT = (((1,), (1,)), ((), ()))
INTERPRET = False


def iota(shape, dim):
    return lax.broadcasted_iota(jnp.int32, shape, dim)


def three_parts(x):
    high = x.astype(BF16).astype(F32)
    rest = x - high
    middle = rest.astype(BF16).astype(F32)
    return high, middle, rest - middle


def merger(index):
    z = (index // PLANE + LINE - FIRST[0]) % LINE
    return z // 4, z % 4, (index + PLANE - FIRST[1]) % PLANE


def pack_kernel(wq_ref, wk_ref, wv_ref, wf_ref, out_ref):
    rows = wq_ref.shape[0]
    stacked = jnp.concatenate(
        [wq_ref[...].astype(F32), wk_ref[...].astype(F32), wv_ref[...].astype(F32), jnp.zeros((rows, wq_ref.shape[1]), F32)],
        axis=0,
    )
    turned = stacked.T.reshape(out_ref.shape)
    forget = jnp.concatenate([jnp.zeros((8, 3 * rows), F32), wf_ref[...].astype(F32)], axis=1)
    lane = iota((1, 8, 128), 2)
    out_ref[...] = jnp.where(lane >= 3 * rows, forget[None], turned).astype(BF16)


def prepare_kernel(
    len_ref, acc_ref, tok_ref, gain_ref, par_ref, bias_ref, gate_ref, head_gain_ref,
    out_ref, link_ref, turned_ref, off_ref, last_ref, bias_out_ref, own_gain_ref, nrm_ref,
):
    rows = gate_ref.shape[2]
    index = lax.axis_index(KV)
    start = index * rows
    nrm_ref[...] = jnp.zeros(nrm_ref.shape, F32)
    gain = gain_ref[...].astype(F32)
    for b in range(4):
        tok = tok_ref[b].astype(F32)
        normed = tok * lax.rsqrt(jnp.mean(tok * tok, axis=1, keepdims=True) + EPSILON) * gain
        for g in range(4):
            at = b * 32 + g * SLOTS
            nrm_ref[at : at + GROUP, :] = normed[g * GROUP : (g + 1) * GROUP]
    for z in range(LINE):
        at = (z + FIRST[0]) % LINE * 128
        features = pltpu.roll(nrm_ref[:, at : at + 128], (PLANE - FIRST[1]) % PLANE * 32, 1)
        out_ref[:, z * 128 : (z + 1) * 128] = features.astype(BF16)

    child = iota((128, 128), 0)
    linked = ((par_ref[...] == child) | (child == iota((128, 128), 1))).astype(F32)
    for _ in range(5):
        low = linked.astype(BF16)
        linked = jnp.minimum(jnp.dot(low, low, preferred_element_type=F32), 1.0)
    link_ref[...] = linked
    turned_ref[...] = linked.T

    lane = iota((8, 128), 1)
    row = iota((8, 128), 0)
    total = jnp.zeros((8, 128), F32)
    offsets = jnp.zeros((8, 128), jnp.int32)
    for s in range(4):
        off = len_ref[s] + acc_ref[s] - start
        offsets = jnp.where(row == s, off, offsets)
        found = jnp.sum(jnp.where(iota((8, rows), 1) == off - 1, gate_ref[s], 0.0), axis=1, keepdims=True)
        high, middle, low = three_parts(jnp.broadcast_to(found, (8, 128)))
        value = jnp.where(lane < 32, high, jnp.where(lane < 64, middle, low))
        total = total + jnp.where((lane % 32 == s * 8 + row) & (lane < 96), value, 0.0)
    off_ref[...] = offsets
    last_ref[...] = jnp.broadcast_to(jnp.sum(total, axis=0, keepdims=True), (8, 128))
    bias_out_ref[...] = jnp.broadcast_to(bias_ref[...], (8, 128))
    own = jnp.where(iota((4, 128), 0) == merger(index)[0], head_gain_ref[...].astype(F32), 0.0)
    own_gain_ref[...] = jnp.broadcast_to(jnp.sum(own, axis=0, keepdims=True), (8, 128))


def project_kernel(x_ref, nrm_ref, bias_ref, piece_ref, gate_ref, wt_ref):
    x = x_ref[...].astype(F32).reshape(16, 4, 8, 128)
    block = iota((128, 128), 1) // 32
    for t in range(4):
        row = None
        for n in range(4):
            moved = x[:, n].reshape(128, 128)
            if n != t:
                moved = pltpu.roll(moved, ((n - t) * 32) % 128, 1)
            row = moved if row is None else jnp.where(block == n, moved, row)
        row = row.reshape(16, 8, 128)
        for m in range(16):
            wt_ref[t * 8 : (t + 1) * 8, m * 128 : (m + 1) * 128] = row[m]
    out = lax.dot_general(wt_ref[...].astype(BF16), nrm_ref[...], NT, preferred_element_type=F32)
    piece = out[:24].reshape(3, 8, 128).astype(BF16)
    piece_ref[...] = jnp.broadcast_to(piece[None], piece_ref.shape)
    pre = out[24:] + bias_ref[...]
    gate_ref[...] = jnp.minimum(pre, 0.0) - jnp.log1p(jnp.exp(-jnp.abs(pre)))


def slot_token(lane):
    return jnp.where(lane % SLOTS < GROUP, (lane % 32) // SLOTS * GROUP + lane % SLOTS, -100000)


def placement(b, off, rows):
    lane = iota((rows, 128), 1)
    return (iota((rows, 128), 0) - off == slot_token(lane)) & (lane // 32 == b)


def columns_of(g_ref, n, start, count):
    parts = [g_ref[y, pl.ds(start, count), n].astype(F32) for y in range(4)]
    return jnp.stack(parts, axis=1).reshape(count * 32, 128)


def attend_kernel(
    off_ref, last_ref, g_ref, k_ref, v_ref, gate_ref, lg_ref, link_ref, turned_ref,
    out_ref, near_ref, climb_ref, q_ref,
):
    rows = k_ref.shape[1]
    q_ref[...] = columns_of(g_ref, 0, 0, 16).T * 0.125
    half = iota((32, 128), 1) < 64
    lane = iota((64, 128), 1)
    row = iota((64, 128), 0)
    mine = (lane % 8 == row % 8) & ((lane // 64) == (row // 32))
    part = (iota((4, 8, 128), 2) % 64) // 8
    slot = iota((4, 8, 128), 1)
    last = last_ref[...][None]

    def scores_of(b):
        found = []
        for p in range(4):
            q = q_ref[b * 32 : (b + 1) * 32, p * 128 : (p + 1) * 128]
            both = jnp.concatenate([jnp.where(half, q, 0.0), jnp.where(half, 0.0, q)], axis=0).astype(BF16)
            found.append(
                lax.dot_general(both, k_ref[b, :, p * 128 : (p + 1) * 128], NT, preferred_element_type=F32)
            )
        return found

    ahead = scores_of(0)
    for b in range(4):
        scores, ahead = ahead, scores_of(b + 1) if b < 3 else None
        off = off_ref[b : b + 1, 0:1]
        gates = jnp.where(iota((8, rows), 1) < off, gate_ref[b], -NEG_LARGE)
        for p in range(4):
            shifts = [jnp.broadcast_to(gates[2 * p + k : 2 * p + k + 1], (32, rows)) for k in range(2)]
            shifted = scores[p] - jnp.concatenate(shifts, axis=0)
            highest = jnp.max(shifted, axis=1, keepdims=True)
            weights = jnp.exp(shifted - highest)
            total = jnp.sum(weights, axis=1, keepdims=True)
            weighted = jnp.dot(
                weights.astype(BF16), v_ref[b, :, p * 128 : (p + 1) * 128], preferred_element_type=F32
            )
            weighted = weighted * (1.0 / total)
            level = jnp.where(mine, highest + jnp.log(total), 0.0)
            level = jnp.sum((level[:32] + level[32:]).reshape(4, 8, 128), axis=1, keepdims=True)
            level = jnp.broadcast_to(jnp.where(off > 0, level, NEG_LARGE), (4, 8, 128))
            high, middle, low = three_parts(level)
            level = jnp.where(part == 0, high, jnp.where(part == 1, middle, low))
            pair = jnp.where(half, weighted[:32], weighted[32:]).reshape(4, 8, 128)
            pair = jnp.where(slot == 6, level, jnp.where(slot == 7, last, pair))
            out_ref[p * 4 : (p + 1) * 4, b] = pair.astype(BF16)

    parts = jnp.concatenate(three_parts(lg_ref[...]), axis=0).astype(BF16)
    summed = jnp.dot(parts, link_ref[...].astype(BF16), preferred_element_type=F32)
    climb = summed[:8] + summed[8:16] + summed[16:]
    climb_ref[...] = climb
    p, group, seq = merger(lax.axis_index(KV))
    half = iota((8, 128), 1) < 64
    at = pl.multiple_of(seq * 32 + group * 8, 8)
    keys = columns_of(g_ref, 1, p * 4, 4).astype(BF16)
    values = columns_of(g_ref, 2, p * 4, 4).astype(BF16)
    q = q_ref[pl.ds(at, 8), pl.ds(pl.multiple_of(p * 128, 128), 128)]
    both = jnp.concatenate([jnp.where(half, q, 0.0), jnp.where(half, 0.0, q)], axis=0).astype(BF16)
    near = jnp.dot(both, keys, preferred_element_type=F32)
    head = iota((8, 128), 0)
    climbs = [jnp.sum(jnp.where(head == 2 * p + k, climb, 0.0), axis=0, keepdims=True) for k in range(2)]
    near = near - jnp.concatenate([jnp.broadcast_to(c, (8, 128)) for c in climbs], axis=0)
    linked = turned_ref[pl.ds(at, 8), :]
    linked = jnp.concatenate([linked, linked], axis=0) > 0.5
    near = jnp.where(linked, near, NEG_LARGE)
    near_top = jnp.max(near, axis=1, keepdims=True)
    near = jnp.where(linked, jnp.exp(near - near_top), 0.0)
    near_sum = jnp.sum(near, axis=1, keepdims=True)
    near = lax.dot_general(near.astype(BF16), values, NT, preferred_element_type=F32)
    near_ref[0] = jnp.where(half, near[:8], near[8:])
    near_ref[1] = jnp.where(half, near_top[:8], near_top[8:])
    near_ref[2] = jnp.where(half, near_sum[:8], near_sum[8:])


def write_kernel(len_ref, acc_ref, g_ref, k_ref, v_ref, kout_ref, vout_ref):
    b = pl.program_id(0)
    rows = k_ref.shape[1]
    off = len_ref[b] + acc_ref[b] - lax.axis_index(KV) * rows
    landing = (off > -24) & (off < rows)

    @pl.when(jnp.logical_not(landing))
    def _():
        kout_ref[0] = k_ref[b]
        vout_ref[0] = v_ref[b]

    @pl.when(landing)
    def _():
        placed = placement(b, off, rows).astype(F32).astype(BF16)
        index = iota((rows, 512), 0)
        landed = (index >= off) & (index < off + 24)
        for n, source, target in ((1, k_ref, kout_ref), (2, v_ref, vout_ref)):
            fresh = columns_of(g_ref, n, 0, 16).astype(BF16)
            written = lax.dot_general(placed, fresh, NT, preferred_element_type=F32)
            target[0] = jnp.where(landed, written, source[b].astype(F32)).astype(BF16)


def merge_kernel(r_ref, near_ref, gain_ref, out_ref, last_ref):
    p, _, seq = merger(lax.axis_index(KV))
    got = r_ref[...].astype(F32)
    lane3 = iota((64, 8, 128), 2)
    keep = (lane3 % 8 == iota((64, 8, 128), 1)) & ((lane3 % 64) // 8 < 3)
    level = jnp.where(keep, got[:, 6:7, :], 0.0).reshape(512, 128).astype(BF16)
    halves = (iota((128, 128), 0) // 64 == iota((128, 128), 1) // 64).astype(F32).astype(BF16)
    level = jnp.dot(level, halves, preferred_element_type=F32).reshape(64, 8, 128)
    top = jnp.max(level, axis=0)
    scale = jnp.exp(level - top[None])
    far_sum = jnp.sum(scale, axis=0)
    far = jnp.sum(scale * got, axis=0)
    whole = jnp.sum(got, axis=0)
    last_ref[...] = whole
    last = whole[7:8]

    half = iota((8, 128), 1) < 64
    lane1 = iota((1, 128), 1)
    first = seq * 8 + 2 * p
    pick = [
        jnp.sum(jnp.where((lane1 % 32 == first + k) & (lane1 < 96), last, 0.0), axis=1, keepdims=True)
        for k in range(2)
    ]
    top = top + jnp.where(half, pick[0], pick[1])
    near, near_top, near_sum = near_ref[0], near_ref[1], near_ref[2]
    overall = jnp.maximum(top, near_top)
    far_scale = jnp.exp(top - overall)
    near_scale = jnp.exp(near_top - overall)
    attended = (far * far_scale + near * near_scale) / (far_sum * far_scale + near_sum * near_scale)
    square = attended * attended
    low = jnp.sum(jnp.where(half, square, 0.0), axis=1, keepdims=True)
    high = jnp.sum(jnp.where(half, 0.0, square), axis=1, keepdims=True)
    mean = jnp.where(half, low, high) * (1.0 / 64.0)
    heads = attended * lax.rsqrt(mean + EPSILON) * gain_ref[...]
    for k in range(3):
        out_ref[:, k] = jnp.broadcast_to(heads[None, 2 * k : 2 * k + 2], (64, 2, 128)).astype(BF16)


def gates_kernel(off_ref, last_ref, climb_ref, gate_ref, gout_ref):
    rows = gate_ref.shape[2]
    last = last_ref[...][7:8]
    lane = iota((32, 128), 1)
    column = jnp.sum(jnp.where((lane % 32 == iota((32, 128), 0)) & (lane < 96), last, 0.0), axis=1, keepdims=True)
    parts = jnp.concatenate(three_parts(climb_ref[...]), axis=0).astype(BF16)
    for b in range(4):
        off = off_ref[b : b + 1, 0:1]
        placed = placement(b, off, rows).astype(F32).astype(BF16)
        written = lax.dot_general(parts, placed, NT, preferred_element_type=F32)
        written = written[:8] + written[8:16] + written[16:] + column[b * 8 : (b + 1) * 8]
        spot = iota((8, rows), 1)
        gout_ref[b] = jnp.where((spot >= off) & (spot < off + 24), written, gate_ref[b])


def mix_kernel(g_ref, w_ref, out_ref, slots_ref):
    slots_ref[...] = jnp.zeros(slots_ref.shape, F32)
    for i in range(64):
        for k in range(3):
            at = i * SLOTS + 2 * k
            slots_ref[at : at + 2, :] = g_ref[i, k].astype(F32)
    total = jnp.zeros((32, 128), F32)
    for p in range(4):
        heads = slots_ref[p * 128 : (p + 1) * 128, :].astype(BF16)
        total = total + lax.dot_general(w_ref[:, p * 128 : (p + 1) * 128], heads, NT, preferred_element_type=F32)
    out_ref[...] = total.reshape(out_ref.shape)


def finish_kernel(x_ref, out_ref):
    width = out_ref.shape[1]
    own = pl.multiple_of(lax.axis_index("tp") * width, width)
    total = x_ref[0, pl.ds(own, width), :]
    for k in range(1, x_ref.shape[0]):
        total = total + x_ref[k, pl.ds(own, width), :]
    for g in range(4):
        for b in range(4):
            at = (g * 4 + b) * SLOTS
            out_ref[b, :, g * GROUP : (g + 1) * GROUP] = total[:, at : at + GROUP]


GRANTS = {body: 16 * 2**20 for body in (project_kernel, attend_kernel, merge_kernel, gates_kernel, write_kernel)}


def spread(array, groups):
    return lax.all_to_all(array, KV, split_axis=0, concat_axis=0, tiled=True, axis_index_groups=groups)


def near_memory(shape, dtype):
    return pltpu.VMEM(shape, dtype)


def here(array):
    return pltpu.with_memory_space_constraint(array, pltpu.VMEM)


def step(
    tokens,
    norm_gain,
    w_query,
    w_key,
    w_value,
    w_forget,
    forget_bias,
    head_gain,
    w_out,
    cache_keys,
    cache_values,
    cache_gates,
    lengths,
    accepted,
    parents,
):
    rows = cache_keys.shape[1]
    pair_count = lax.axis_size("tp")
    smem = pl.BlockSpec(memory_space=pltpu.SMEM)
    vmem = pl.BlockSpec(memory_space=pltpu.VMEM)

    def kernel(body, out_shape, **kw):
        params = pltpu.CompilerParams(vmem_limit_bytes=GRANTS.get(body))
        return pl.pallas_call(body, out_shape=out_shape, interpret=INTERPRET, compiler_params=params, **kw)

    packed = kernel(pack_kernel, near_memory((64, 8, 128), BF16))(w_query, w_key, w_value, w_forget.T)
    columns = spread(packed, ALL)

    groups = parents.reshape(4, 4, GROUP)
    groups = jnp.where(
        groups < 0, -1, groups // GROUP * SLOTS + groups % GROUP + 32 * jnp.arange(4, dtype=jnp.int32)[:, None, None]
    )
    slots = jnp.pad(groups, ((0, 0), (0, 0), (0, SLOTS - GROUP)), constant_values=-1).reshape(1, 128)
    gates = here(cache_gates)
    keys = here(cache_keys)
    values = here(cache_values)
    small = near_memory((8, 128), F32)
    normed, link, turned, offsets, last_part, bias, own_gain = kernel(
        prepare_kernel,
        (
            near_memory((128, 2048), BF16),
            near_memory((128, 128), F32),
            near_memory((128, 128), F32),
            near_memory((8, 128), jnp.int32),
            small,
            small,
            small,
        ),
        in_specs=[smem, smem] + [vmem] * 6,
        scratch_shapes=[pltpu.VMEM((128, 2048), F32)],
    )(
        lengths,
        accepted,
        tokens,
        norm_gain.reshape(1, -1),
        slots,
        forget_bias.reshape(8, 1),
        gates,
        head_gain.reshape(4, 128),
    )
    pieces, log_gate = kernel(
        project_kernel,
        (near_memory((16, 3, 8, 128), BF16), small),
        scratch_shapes=[pltpu.VMEM((32, 2048), F32)],
    )(here(columns), here(normed), here(bias))
    line = spread(pieces, LINES)
    plane = here(spread(jnp.broadcast_to(line[None], (4, *line.shape)), PLANES))

    partial, near, climb = kernel(
        attend_kernel,
        (near_memory((16, 4, 8, 128), BF16), near_memory((3, 8, 128), F32), small),
        scratch_shapes=[pltpu.VMEM((128, 512), F32)],
    )(
        here(offsets),
        here(last_part),
        plane,
        keys,
        values,
        gates,
        here(log_gate),
        here(link),
        here(turned),
    )
    received = spread(partial.reshape(64, 8, 128), ALL)
    heads, last = kernel(merge_kernel, (near_memory((64, 3, 2, 128), BF16), small))(
        here(received), here(near), here(own_gain)
    )
    everyone = spread(heads, ALL)
    cache_spec = pl.BlockSpec((1, rows, 512), lambda b: (b, 0, 0))
    keys_out, values_out = kernel(
        write_kernel,
        (
            jax.ShapeDtypeStruct(cache_keys.shape, BF16),
            jax.ShapeDtypeStruct(cache_values.shape, BF16),
        ),
        grid=(4,),
        in_specs=[smem, smem, vmem, vmem, vmem],
        out_specs=(cache_spec, cache_spec),
    )(lengths, accepted, plane, keys, values)
    gates_out = kernel(gates_kernel, jax.ShapeDtypeStruct(cache_gates.shape, F32))(
        here(offsets), here(last), here(climb), gates
    )

    share = kernel(mix_kernel, near_memory((32, 128), F32), scratch_shapes=[pltpu.VMEM((512, 128), F32)])(
        here(everyone), here(w_out.T)
    )
    shares = lax.all_gather(share, "tp")
    mixed = kernel(finish_kernel, jax.ShapeDtypeStruct((4, 32 // pair_count, 24), F32))(here(shares))
    mixed = jnp.swapaxes(mixed, 1, 2)
    return (mixed, keys_out, values_out, gates_out)


def solution(mesh):
    torus = Mesh(
        mesh.devices.reshape(mesh.shape["dp"], LINE * PLANE, mesh.shape["tp"]),
        ("dp", "kv", "tp"),
    )
    return jax.shard_map(
        step,
        mesh=torus,
        in_specs=(
            P("dp", None, None),
            P(),
            P(KV, "tp"),
            P(KV, "tp"),
            P(KV, "tp"),
            P(KV, "tp"),
            P("tp"),
            P("tp"),
            P("tp", KV),
            P("dp", KV, "tp"),
            P("dp", KV, "tp"),
            P("dp", "tp", KV),
            P("dp"),
            P("dp"),
            P("dp", None),
        ),
        out_specs=(P("dp", None, KV_TP), P("dp", KV, "tp"), P("dp", KV, "tp"), P("dp", "tp", KV)),
        check_vma=False,
    )
```
